32 devices in a mesh: fs: 4 (over y, x), tp: 8 (over z, core).
Axes of the slice: x: 2, y: 2, z: 4, core: 2. Of those that a mesh axis runs over, the one named last changes fastest.
Arguments:
- inputs: bfloat16 [1536, 2048], P('fs'), may hold values from -6 to 6
- pre_act: bfloat16 [1536, 8192], P('fs', 'tp'), may hold values from -6 to 6
- cotangent: bfloat16 [1536, 2048], P('fs'), may hold values from -6 to 6
- up_weight: bfloat16 [2048, 8192], P('fs', 'tp'), may hold values from -0.125 to 0.125
- down_weight: bfloat16 [8192, 2048], P('tp', 'fs'), may hold values from -0.0625 to 0.0625
Outputs:
- input_grad: bfloat16 [1536, 2048], P('fs')
- up_grad: float32 [2048, 8192], P('fs', 'tp')
- down_grad: float32 [8192, 2048], P('tp', 'fs')
- up_norms: float32 [2048], P('fs')
- down_norms: float32 [8192], P('tp')
The draws below stay inside these ranges and needn't reach their ends.
All inputs are finite; a program needn't handle non-finite values.
Results may differ from the reference program's by a relative error of at most 0.0051.
Values may be sent and summed in bfloat16 or wider, within the bound.
A program may use at most 64 MiB of HBM per device.

```python
import jax
import jax.numpy as jnp

D = 2048
FF = 8192
TOKENS = 1536


def raised(drawn, key, source, target, shards_of, factor):
    def block_of(position):
        return (jnp.arange(drawn.shape[position]) // (drawn.shape[position] // shards_of)).reshape((-1,) + (1,) * (drawn.ndim - 1 - position))

    near = jax.random.permutation(key, shards_of)[block_of(target)]
    other_side = (block_of(target) + shards_of // 2) % shards_of
    return jnp.where((block_of(source) == near) | (block_of(source) == other_side), factor * drawn, drawn)


def steps_of(own_key, extent, cuts, low, top_value):
    def one(position, blocks):
        steps = jax.random.uniform(jax.random.fold_in(jax.random.fold_in(own_key, 6), position), (blocks,), jnp.float32, low / len(cuts), top_value / len(cuts))
        return jnp.repeat(jnp.exp(steps), extent[position] // blocks).reshape((-1,) + (1,) * (len(extent) - position - 1))

    level = one(*cuts[0])
    for cut in cuts[1:]:
        level = level * one(*cut)
    return level


def normal_values(stream_key, shape, width, most, pieces=(), held_as=jnp.bfloat16):
    entries = jax.random.normal(stream_key, shape, jnp.float32) * width
    if len(pieces) > 0:
        entries = steps_of(stream_key, shape, pieces, -0.22, 0.18) * entries
    return jnp.clip(entries, min=-most, max=most).astype(held_as)


def noise_with(own_key, dims, scale, most, cuts, heavy, held_as=jnp.bfloat16):
    result = scale * jax.random.normal(own_key, dims, jnp.float32)
    if cuts:
        result = result * steps_of(own_key, dims, cuts, -0.22, 0.18)
    return jnp.clip(raised(result, jax.random.fold_in(own_key, 3), *heavy), -most, most).astype(held_as)


def setup_inputs(seed: int = 0) -> dict:
    key_list = jax.random.split(jax.random.key(seed), 6)
    return {
        "inputs": noise_with(key_list[0], (TOKENS, D), 1.0, 6.0, ((0, 4),), (0, 1, 4, 2.0)),
        "pre_act": normal_values(key_list[1], (TOKENS, FF), 1.0, 6.0, ((0, 4), (1, 8))),
        "cotangent": noise_with(key_list[2], (TOKENS, D), 1.0, 6.0, ((0, 4),), (0, 1, 4, 2.0)),
        "up_weight": normal_values(key_list[3], (D, FF), D ** -0.5, 0.125, ((0, 4), (1, 8))),
        "down_weight": normal_values(key_list[4], (FF, D), FF ** -0.5, 0.0625, ((0, 8), (1, 4))),
    }


def reference(inputs, pre_act, cotangent, up_weight, down_weight):
    active = jnp.maximum(pre_act.astype(jnp.float32), 0.0)
    squared = (active * active).astype(jnp.bfloat16)
    sq_grad = jnp.dot(cotangent, down_weight.T, preferred_element_type=jnp.float32)
    pre_grad = (2.0 * active * sq_grad).astype(jnp.bfloat16)
    input_grad = jnp.dot(pre_grad, up_weight.T, preferred_element_type=jnp.float32).astype(jnp.bfloat16)
    up_grad = jnp.dot(inputs.T, pre_grad, preferred_element_type=jnp.float32)
    down_grad = jnp.dot(squared.T, cotangent, preferred_element_type=jnp.float32)
    up_norms = jnp.sum(up_grad * up_grad, axis=1)
    down_norms = jnp.sum(down_grad * down_grad, axis=1)
    return input_grad, up_grad, down_grad, up_norms, down_norms
```

```python
import functools

import jax
import jax.numpy as jnp
from jax import lax
from jax.experimental import pallas as pl
from jax.experimental.pallas import tpu as pltpu
from jax.sharding import PartitionSpec as P

MESH = pl.DeviceIdType.MESH
F32, BF16 = jnp.float32, jnp.bfloat16


def contract_last(left, right):
    return lax.dot_general(left, right, (((1,), (1,)), ((), ())), preferred_element_type=F32)


def contract_first(left, right):
    return lax.dot_general(left, right, (((0,), (0,)), ((), ())), preferred_element_type=F32)


def bits_of(n):
    return [1 << i for i in range(n.bit_length() - 1)]


def by_weight(n, down=False):
    return sorted(range(1, n), key=lambda m: (bin(m).count("1"), -m if down else m))


class Gather:
    def __init__(self, n, me, device, source, place, send, recv, orders):
        self.n, self.me, self.device = n, me, device
        self.source, self.place = source, place
        self.send, self.recv, self.orders = send, recv, orders
        self.started = []

    def targets(self, cls, m):
        bits = bits_of(self.n)
        if m == 0:
            return bits
        if self.orders[cls] == "up":
            return [b for b in bits if b > m]
        return [b for b in bits if b < (m & -m)]

    def copy(self, cls, m, b):
        there = self.place(self.me ^ m, cls)
        return pltpu.make_async_remote_copy(
            src_ref=self.source(cls) if m == 0 else there,
            dst_ref=there,
            send_sem=self.send(cls, m ^ b),
            recv_sem=self.recv(cls, m ^ b),
            device_id=self.device(self.me ^ b),
            device_id_type=MESH,
        )

    def push(self, cls, m, only=None):
        for b in self.targets(cls, m):
            if only is None or b == only:
                copy = self.copy(cls, m, b)
                copy.start()
                self.started.append(copy)

    def push_own(self, turns=None):
        classes = list(range(len(self.orders)))
        for i, b in enumerate(bits_of(self.n)):
            for j, cls in enumerate(classes if i % 2 == 0 else classes[::-1]):
                if turns is None or j in turns:
                    self.push(cls, 0, b)

    def arrive(self, cls, m):
        here = self.place(self.me ^ m, cls)
        pltpu.make_async_remote_copy(
            src_ref=here,
            dst_ref=here,
            send_sem=self.send(cls, m),
            recv_sem=self.recv(cls, m),
            device_id=self.device(self.me ^ (m & -m)),
            device_id_type=MESH,
        ).wait_recv()

    def drain(self):
        for copy in self.started:
            copy.wait_send()


def share_rows(rows, parts):
    cuts = 1
    while cuts < parts and rows % (2 * cuts * 16) == 0:
        cuts *= 2
    return cuts


def piece_shape(nt, rows, db):
    nz = nt // 2
    if db % (128 * nz) == 0:
        return rows // 2, db // nz
    return rows // nt, db


def fused_kernel(nf, nt, subs, strips, cot, dw, pa, inp, up, ugrad, dgrad, got, un_all, dn_all,
                 cot_all, dw_all, pa_all, inp_all, up_all, pre, sqr, sq,
                 part, from_sib, wire, landed, final, un_own, dn_own,
                 xs, xr, zs, zr, ss, sr, a_s, a_r, bs, br, hs, hr, ws, wr, ts, tr, gs, gr, ks, kr,
                 us, ur, ds, dr, local_sem):
    f, t = lax.axis_index("fs"), lax.axis_index("tp")
    z, c = t // 2, t % 2
    nz = nt // 2
    rows, d = cot.shape
    ff, db = dw.shape
    half = rows // subs
    pr, pc = part.shape[3:]
    own_cols = pl.ds(pl.multiple_of(f * db, db), db)

    def remote(src, dst, send, recv, device):
        return pltpu.make_async_remote_copy(src_ref=src, dst_ref=dst, send_sem=send, recv_sem=recv,
                                            device_id=device, device_id_type=MESH)

    def columns(g, side):
        ih = rows // 2
        return inp.at[pl.ds(pl.multiple_of(side * ih, ih), ih), pl.ds(pl.multiple_of(g * db, db), db)]

    def in_half(g, side):
        ih = rows // 2
        return inp_all.at[g, pl.ds(pl.multiple_of(side * ih, ih), ih), :]

    own = [
        pltpu.make_async_copy(dw, dw_all.at[:, own_cols], local_sem.at[0]),
        pltpu.make_async_copy(cot, cot_all.at[f], local_sem.at[1]),
        pltpu.make_async_copy(pa, pa_all.at[f], local_sem.at[2]),
        pltpu.make_async_copy(up, up_all, local_sem.at[3]),
        pltpu.make_async_copy(columns(f, 0), in_half(f, 0), local_sem.at[4]),
        pltpu.make_async_copy(columns(f, 1), in_half(f, 1), local_sem.at[5]),
    ]
    for copy in own:
        copy.start()

    barrier = pltpu.get_barrier_semaphore()
    peers = [(f ^ m, t) for m in range(1, nf)] + [(f, t ^ m) for m in range(1, nt)]
    for peer in peers:
        pl.semaphore_signal(barrier, inc=1, device_id=peer, device_id_type=MESH)
    pl.semaphore_wait(barrier, len(peers))

    row_cuts = share_rows(rows, nt)
    col_cuts = nt // row_cuts
    cr, cc = rows // row_cuts, d // col_cuts

    def piece(ref, y, h=None):
        row = pl.multiple_of((y // col_cuts) * cr, cr)
        width = cc if h is None else cc // 2
        col = (y % col_cuts) * cc + (0 if h is None else h * width)
        return ref.at[pl.ds(row, cr), pl.ds(pl.multiple_of(col, width), width)]

    dwh = ff // 2
    pah = rows // 2

    def over_fs(k, source, place):
        return Gather(nf, f, lambda g: (g, t), source, place,
                      lambda cls, m: xs.at[k, cls, m], lambda cls, m: xr.at[k, cls, m], ("up", "down"))

    g_cot = over_fs(0, lambda h: piece(cot, t, h), lambda g, h: piece(cot_all.at[g], t, h))
    g_dw = over_fs(1, lambda h: dw.at[pl.ds(h * dwh, dwh), :],
                   lambda g, h: dw_all.at[pl.ds(h * dwh, dwh), pl.ds(pl.multiple_of(g * db, db), db)])
    g_pa = over_fs(2, lambda h: pa.at[pl.ds(h * pah, pah), :],
                   lambda g, h: pa_all.at[g, pl.ds(h * pah, pah), :])

    def strip(m, s, y):
        return piece(cot_all.at[f ^ m], y, s if strips == 2 else None)

    def over_z(m, s):
        spot = lambda y, cls=0: strip(m, s, 2 * y + c)
        return Gather(nz, z, lambda y: (f, 2 * y + c), lambda cls: spot(z), spot,
                      lambda cls, k: zs.at[m, s, k], lambda cls, k: zr.at[m, s, k], ("down",))

    def to_sibling(m, s, k):
        spot = strip(m, s, 2 * (z ^ k) + c)
        return remote(spot, spot, ss.at[m, s, k], sr.at[m, s, k], (f, t ^ 1))

    def from_sibling(m, s, k):
        spot = strip(m, s, 2 * (z ^ k) + 1 - c)
        return remote(spot, spot, ss.at[m, s, k], sr.at[m, s, k], (f, t ^ 1))

    exchange = lambda m: remote(columns(f ^ m, c), in_half(f, c), a_s.at[m], a_r.at[m], (f ^ m, t))
    exchanged = lambda m: remote(in_half(f ^ m, c), in_half(f ^ m, c), a_s.at[m], a_r.at[m], (f ^ m, t))
    in_to = lambda m: remote(in_half(f ^ m, c), in_half(f ^ m, c), bs.at[m], br.at[m], (f, t ^ 1))
    in_from = lambda m: remote(in_half(f ^ m, 1 - c), in_half(f ^ m, 1 - c), bs.at[m], br.at[m], (f, t ^ 1))

    masks = by_weight(nf)
    zorder = by_weight(nz, True)
    left = {m: 2 for m in masks}
    rings = {(m, s): over_z(m, s) for m in masks for s in range(strips)}
    singles = [m for m in masks if m & (m - 1) == 0]
    pairs = [(m, cls) for m in masks for cls in (0, 1)]
    inner = [p for p in pairs if g_dw.targets(p[1], p[0])]
    outer = [p for p in pairs if p not in inner]

    def take_cot(items):
        for m, cls in items:
            g_cot.arrive(cls, m)
            g_cot.push(cls, m)
            left[m] -= 1
            if strips == 2:
                rings[m, cls].push(0, 0)
                to_sibling(m, cls, 0).start()
            elif left[m] == 0:
                rings[m, 0].push(0, 0)
                to_sibling(m, 0, 0).start()

    def turn(m, s, steps):
        for k in steps:
            rings[m, s].arrive(0, k)
            rings[m, s].push(0, k)
            to_sibling(m, s, k).start()

    def take(g, items):
        for m, cls in items:
            g.arrive(cls, m)
            g.push(cls, m)

    tile = min(ff, 256)

    def square_grad(m):
        g = f ^ m
        if m:
            for s in range(strips):
                for k in range(nz):
                    from_sibling(m, s, k).wait_recv()
        sq[g] = contract_last(cot_all[g], dw_all[...])

    def unit(u):
        m, h = u
        g = f ^ m
        i = m * subs + h
        some = pl.ds(h * half, half)
        for j in range(ff // tile):
            cols = pl.ds(j * tile, tile)
            active = jnp.maximum(pa_all[g, some, cols].astype(F32), 0.0)
            pre[g, some, cols] = (2.0 * active * sq[g, some, cols]).astype(BF16)
            sqr[g, some, cols] = (active * active).astype(BF16)
        total = contract_last(pre[g, some, :], up_all[...])
        wide = half // 2 == pr
        for k in range(nt):
            row, col = ((k % 2) * pr, (k // 2) * pc) if wide else (k * pr, 0)
            part[i, k % 2, k // 2] = total[row:row + pr, col:col + pc]
        halves(i).start()

    def halves(i):
        return remote(part.at[i, 1 - c], from_sib.at[i], hs.at[i], hr.at[i], (f, t ^ 1))

    def spread(i, k):
        return remote(wire.at[i, k], landed.at[i, k], ws.at[i, k], wr.at[i, k], (f, 2 * (z ^ k) + c))

    def scatter(u):
        i = u[0] * subs + u[1]
        halves(i).wait_recv()
        for k in range(nz - 1, 0, -1):
            wire[i, k] = (part[i, c, z ^ k] + from_sib[i, z ^ k]).astype(BF16)
            spread(i, k).start()

    def trade(u):
        i = u[0] * subs + u[1]
        return remote(final.at[i], got.at[u[1], f, t], ts.at[i], tr.at[i], (f ^ u[0], t))

    def traded(u):
        i = u[0] * subs + u[1]
        spot = got.at[u[1], f ^ u[0], t]
        return remote(spot, spot, ts.at[i], tr.at[i], (f ^ u[0], t))

    def finish(u):
        m, h = u
        i = m * subs + h
        value = part[i, c, z] + from_sib[i, z]
        for k in range(1, nz):
            spread(i, k).wait_recv()
            value = value + landed[i, k].astype(F32)
        if m == 0:
            got[h, f, t] = value.astype(BF16)
        else:
            final[i] = value.astype(BF16)
            trade(u).start()

    def ahead(u, k):
        i = u[0] * subs + u[1]
        spot = got.at[u[1], f ^ u[0], t]
        return remote(spot, spot, gs.at[i, k], gr.at[i, k], (f, t ^ (2 * k)))

    def came(u, k):
        i = u[0] * subs + u[1]
        spot = got.at[u[1], f ^ u[0], t ^ (2 * k)]
        return remote(spot, spot, gs.at[i, k], gr.at[i, k], (f, t ^ (2 * k)))

    def over(u, k, mine=True):
        i = u[0] * subs + u[1]
        spot = got.at[u[1], f ^ u[0], (t if mine else t ^ 1) ^ (2 * k)]
        return remote(spot, spot, ks.at[i, k], kr.at[i, k], (f, t ^ 1))

    def announce(u):
        if u[0]:
            traded(u).wait_recv()
        for k in range(nz - 1, 0, -1):
            ahead(u, k).start()
        over(u, 0).start()

    def relay(u):
        for k in range(1, nz):
            came(u, k).wait_recv()
            over(u, k).start()

    def down(m, first):
        g = f ^ m
        value = contract_first(sqr[g], cot_all[g, :, own_cols])
        dgrad[...] = value if first else dgrad[...] + value

    def up_part(m, first):
        g = f ^ m
        value = contract_first(inp_all[g], pre[g])
        ugrad[...] = value if first else ugrad[...] + value

    single = lambda p: p[0] in singles
    near = [p for p in inner if single(p)] + [p for p in outer if single(p)]
    far = [p for p in pairs if not single(p)]
    ahead_k = [k for k in zorder if rings[masks[0], 0].targets(0, k)]
    end_k = [k for k in zorder if k not in ahead_k]
    spots = lambda items: [p for p in items if p[1] < strips]
    near_spots, far_spots = spots(near), spots(far)

    g_cot.push_own()
    g_dw.push_own((0,))
    take_cot(near)
    g_dw.push_own((1,))
    for m, s in near_spots[:2]:
        turn(m, s, ahead_k)
    take(g_dw, inner)
    g_pa.push_own()
    take_cot(far)
    for m, s in near_spots[2:]:
        turn(m, s, ahead_k)
    for m, s in near_spots:
        turn(m, s, end_k)
    for m, s in far_spots:
        turn(m, s, ahead_k)
    take(g_dw, outer)
    for copy in own:
        copy.wait()

    middle = [p for p in outer if single(p)]
    last = [p for p in outer if not single(p)]
    pieces = inner, middle, last
    if subs == 1:
        inner, middle, last = [], [(m, 0) for m in singles], [(m, 0) for m in masks if m not in singles]
    first_units = [(0, h) for h in range(subs)]
    square_grad(0)
    for u in first_units:
        unit(u)
    for m, s in far_spots:
        turn(m, s, end_k)
    square_grad(singles[0])
    for u in first_units:
        scatter(u)
    for m in singles[1:]:
        square_grad(m)
    for u in first_units:
        finish(u)
        announce(u)

    def come(items):
        for m, cls in items:
            g_pa.arrive(cls, m)

    def forward(items):
        for m, cls in items:
            g_pa.push(cls, m)

    come(pieces[0])
    if subs == 1:
        forward(pieces[0])
    for u in inner:
        unit(u)
    for m in masks:
        if m not in singles:
            square_grad(m)
    for u in inner:
        scatter(u)
    down(0, True)
    for u in first_units:
        relay(u)
    up_part(0, True)
    for u in inner:
        finish(u)
    if subs == 2:
        forward(pieces[0])
    take(g_pa, pieces[1])
    for u in middle:
        unit(u)
    for u in inner:
        announce(u)
    for u in middle:
        scatter(u)
    for m in singles:
        down(m, False)
    for u in middle:
        finish(u)
    for m in masks:
        exchange(m).start()
    for u in inner:
        relay(u)
    for p, u in zip(pieces[2], last) if subs == 2 else []:
        come([p])
        unit(u)
    if subs == 1:
        take(g_pa, pieces[2])
        for u in last:
            unit(u)
    for u in last:
        scatter(u)
    for u in middle:
        announce(u)
    for m in masks:
        if m not in singles:
            down(m, False)
    dn_own[...] = jnp.sum(dgrad[...] * dgrad[...], axis=1).reshape(1, ff)
    for u in last:
        finish(u)
    downs = [remote(dn_own, dn_all.at[f], ds.at[m], dr.at[m], (f ^ m, t)) for m in range(1, nf)]
    for copy in downs:
        copy.start()
    for m in masks:
        exchanged(m).wait_recv()
        in_to(m).start()
    for u in last:
        announce(u)
    for u in middle:
        relay(u)
    for m in masks:
        in_from(m).wait_recv()
        up_part(m, False)
    un_own[...] = jnp.sum(ugrad[...] * ugrad[...], axis=1).reshape(1, db)
    ups = [remote(un_own, un_all.at[t], us.at[m], ur.at[m], (f, t ^ m)) for m in range(1, nt)]
    for copy in ups:
        copy.start()
    for u in last:
        relay(u)

    dn_all[f] = dn_own[...]
    un_all[t] = un_own[...]
    for m in range(1, nf):
        remote(dn_all.at[f ^ m], dn_all.at[f ^ m], ds.at[m], dr.at[m], (f ^ m, t)).wait_recv()
    for m in range(1, nt):
        remote(un_all.at[t ^ m], un_all.at[t ^ m], us.at[m], ur.at[m], (f, t ^ m)).wait_recv()
    units = first_units + inner + middle + last
    for u in units:
        for k in range(nz):
            over(u, k, False).wait_recv()

    for u in units:
        i = u[0] * subs + u[1]
        halves(i).wait_send()
        for k in range(1, nz):
            spread(i, k).wait_send()
            ahead(u, k).wait_send()
        for k in range(nz):
            over(u, k).wait_send()
        if u[0]:
            trade(u).wait_send()
    for m in masks:
        for s in range(strips):
            for k in range(nz):
                to_sibling(m, s, k).wait_send()
            rings[m, s].drain()
        in_to(m).wait_send()
        exchange(m).wait_send()
    for g in (g_cot, g_dw, g_pa):
        g.drain()
    for copy in ups + downs:
        copy.wait_send()


def fused(nf, nt, cot, dw, pa, inp, up):
    rows, d = inp.shape
    ff, db = dw.shape
    nz = nt // 2
    subs = strips = 2 if nf * nz <= 64 else 1
    half = rows // subs
    pr, pc = piece_shape(nt, half, db)
    units = nf * subs
    dma = pltpu.SemaphoreType.DMA
    vmem = pl.BlockSpec(memory_space=pltpu.VMEM)
    hbm = pl.BlockSpec(memory_space=pl.ANY)
    V = pltpu.VMEM
    sems = [dma((3, 2, nf))] * 2 + [dma((nf, strips, nz))] * 4 + [dma((nf,))] * 4
    sems += [dma((units,))] * 2 + [dma((units, nz))] * 2 + [dma((units,))] * 2 + [dma((units, nz))] * 4
    sems += [dma((nt,))] * 2 + [dma((nf,))] * 2 + [dma((6,))]
    return pl.pallas_call(
        functools.partial(fused_kernel, nf, nt, subs, strips),
        out_shape=[
            V((db, ff), F32), V((ff, db), F32), V((subs, nf, nt, pr, pc), BF16),
            V((nt, 1, db), F32), V((nf, 1, ff), F32),
        ],
        in_specs=[hbm] * 5,
        out_specs=[vmem] * 5,
        scratch_shapes=[
            V((nf, rows, d), BF16), V((ff, d), BF16), V((nf, rows, ff), BF16), V((nf, rows, db), BF16),
            V((db, ff), BF16), V((nf, rows, ff), BF16), V((nf, rows, ff), BF16), V((nf, rows, ff), F32),
            V((units, 2, nz, pr, pc), F32), V((units, nz, pr, pc), F32),
            V((units, nz, pr, pc), BF16), V((units, nz, pr, pc), BF16), V((units, pr, pc), BF16),
            V((1, db), F32), V((1, ff), F32),
        ] + sems,
        compiler_params=pltpu.CompilerParams(has_side_effects=True, collective_id=0, vmem_limit_bytes=54 * 2 ** 20),
    )(cot, dw, pa, inp, up)


def deliver_kernel(ugrad, dgrad, got, un_all, dn_all, ug_out, dg_out, out, un_out, dn_out, whole, un_sum, dn_sum, sem):
    subs, nf, nt, pr, pc = got.shape
    rows, d = whole.shape
    half, db = rows // subs, d // nf
    copies = [pltpu.make_async_copy(ugrad, ug_out, sem.at[0]), pltpu.make_async_copy(dgrad, dg_out, sem.at[1])]
    for copy in copies:
        copy.start()
    wide = half // 2 == pr
    for h in range(subs):
        for k in range(nt):
            for g in range(nf):
                row, col = ((k % 2) * pr, (k // 2) * pc) if wide else (k * pr, 0)
                whole[h * half + row:h * half + row + pr, g * db + col:g * db + col + pc] = got[h, g, k]
    un, dn = un_all[0], dn_all[0]
    for k in range(1, nt):
        un = un + un_all[k]
    for k in range(1, nf):
        dn = dn + dn_all[k]
    un_sum[...] = un
    dn_sum[...] = dn
    last = [pltpu.make_async_copy(whole, out, sem.at[2]), pltpu.make_async_copy(un_sum, un_out, sem.at[3]),
            pltpu.make_async_copy(dn_sum, dn_out, sem.at[4])]
    for copy in last:
        copy.start()
    for copy in copies + last:
        copy.wait()


def deliver(rows, d, ugrad, dgrad, got, un_all, dn_all):
    hbm, vmem = pl.BlockSpec(memory_space=pl.ANY), pl.BlockSpec(memory_space=pltpu.VMEM)
    V = pltpu.VMEM
    un, dn = un_all.shape[1:], dn_all.shape[1:]
    H = jax.ShapeDtypeStruct
    return pl.pallas_call(
        deliver_kernel,
        out_shape=[H(ugrad.shape, F32), H(dgrad.shape, F32), H((rows, d), BF16), H(un, F32), H(dn, F32)],
        in_specs=[vmem] * 5,
        out_specs=[hbm] * 5,
        scratch_shapes=[V((rows, d), BF16), V(un, F32), V(dn, F32), pltpu.SemaphoreType.DMA((5,))],
        compiler_params=pltpu.CompilerParams(vmem_limit_bytes=16 * 2 ** 20),
    )(ugrad, dgrad, got, un_all, dn_all)


def local(nf, nt, inputs, pre_act, cotangent, up_weight, down_weight):
    db, ff = up_weight.shape
    parts = fused(nf, nt, cotangent, down_weight, pre_act, inputs, up_weight)
    up_grad, down_grad, out, un, dn = deliver(*inputs.shape, *parts)
    return out, up_grad, down_grad, un.reshape(db), dn.reshape(ff)


def solution(mesh):
    in_specs = (P("fs", None), P("fs", "tp"), P("fs", None), P("fs", "tp"), P("tp", "fs"))
    out_specs = (P("fs", None), P("fs", "tp"), P("tp", "fs"), P("fs"), P("tp"))
    body = functools.partial(local, mesh.shape["fs"], mesh.shape["tp"])
    return jax.shard_map(body, mesh=mesh, in_specs=in_specs, out_specs=out_specs, check_vma=False)
```

```python
import functools

import jax
import jax.numpy as jnp
from jax import lax
from jax.experimental import pallas as pl
from jax.experimental.pallas import tpu as pltpu
from jax.sharding import PartitionSpec as P

MESH = pl.DeviceIdType.MESH
F32, BF16 = jnp.float32, jnp.bfloat16


def contract_last(left, right):
    return lax.dot_general(left, right, (((1,), (1,)), ((), ())), preferred_element_type=F32)


def contract_first(left, right):
    return lax.dot_general(left, right, (((0,), (0,)), ((), ())), preferred_element_type=F32)


def bits_of(n):
    return [1 << i for i in range(n.bit_length() - 1)]


def by_weight(n, down=False):
    return sorted(range(1, n), key=lambda m: (bin(m).count("1"), -m if down else m))


class Gather:
    def __init__(self, n, me, device, source, place, send, recv, orders):
        self.n, self.me, self.device = n, me, device
        self.source, self.place = source, place
        self.send, self.recv, self.orders = send, recv, orders

    def targets(self, cls, m):
        bits = bits_of(self.n)
        if self.orders[cls] == "flat":
            return list(range(self.n - 1, 0, -1)) if m == 0 else []
        if m == 0:
            return bits
        if self.orders[cls] == "up":
            return [b for b in bits if b > m]
        return [b for b in bits if b < (m & -m)]

    def copy(self, cls, m, b):
        there = self.place(self.me ^ m, cls)
        return pltpu.make_async_remote_copy(
            src_ref=self.source(cls) if m == 0 else there,
            dst_ref=there,
            send_sem=self.send,
            recv_sem=self.recv(cls, m ^ b),
            device_id=self.device(self.me ^ b),
            device_id_type=MESH,
        )

    def push(self, cls, m, only=None):
        for b in self.targets(cls, m):
            if only is None or b == only:
                self.copy(cls, m, b).start()

    def push_own(self, turns=None):
        classes = list(range(len(self.orders)))
        for i, b in enumerate(bits_of(self.n)):
            for j, cls in enumerate(classes if i % 2 == 0 else classes[::-1]):
                if turns is None or j in turns:
                    self.push(cls, 0, b)

    def arrive(self, cls, m):
        here = self.place(self.me ^ m, cls)
        pltpu.make_async_remote_copy(
            src_ref=here,
            dst_ref=here,
            send_sem=self.send,
            recv_sem=self.recv(cls, m),
            device_id=self.device(self.me ^ (m & -m)),
            device_id_type=MESH,
        ).wait_recv()

    def drain(self, sent):
        pltpu.make_async_remote_copy(src_ref=sent, dst_ref=sent, send_sem=self.send, recv_sem=self.send,
                                     device_id=self.device(self.me ^ 1), device_id_type=MESH).wait_send()


def share_rows(rows, parts):
    cuts = 1
    while cuts < parts and rows % (2 * cuts * 16) == 0:
        cuts *= 2
    return cuts


def piece_shape(nt, rows, db):
    nz = nt // 2
    if db % (128 * nz) == 0:
        return rows // 2, db // nz
    return rows // nt, db


def fused_kernel(nf, nt, subs, strips, cot, dw, pa, inp, up, ugrad, dgrad, got, un_all, dn_all,
                 cot_all, dw_all, pa_all, inp_all, up_all, pre, sqr, sq,
                 part, from_sib, wire, landed, final, un_own, dn_own,
                 xs, xr, pa_r, zs, zr, ss, sr, a_s, a_r, bs, br, hs, hr, ws, wr, ts, tr, gs, gr, ks, kr,
                 us, ur, ds, dr, local_sem):
    f, t = lax.axis_index("fs"), lax.axis_index("tp")
    z, c = t // 2, t % 2
    nz = nt // 2
    rows, d = cot.shape
    ff, db = dw.shape
    height = rows // subs
    pr, pc = part.shape[3:]
    own_cols = pl.ds(pl.multiple_of(f * db, db), db)

    def remote(src, dst, send, recv, device):
        return pltpu.make_async_remote_copy(src_ref=src, dst_ref=dst, send_sem=send, recv_sem=recv,
                                            device_id=device, device_id_type=MESH)

    ih = rows // 2

    def columns(g, side):
        return inp.at[pl.ds(pl.multiple_of(side * ih, ih), ih), pl.ds(pl.multiple_of(g * db, db), db)]

    def in_half(g, side):
        return inp_all.at[g, pl.ds(pl.multiple_of(side * ih, ih), ih), :]

    own = [
        pltpu.make_async_copy(cot, cot_all.at[f], local_sem.at[0]),
        pltpu.make_async_copy(dw, dw_all.at[:, own_cols], local_sem.at[1]),
        pltpu.make_async_copy(pa, pa_all.at[f], local_sem.at[2]),
        pltpu.make_async_copy(up, up_all, local_sem.at[3]),
        pltpu.make_async_copy(inp.at[:, own_cols], inp_all.at[f], local_sem.at[4]),
    ]
    for copy in own:
        copy.start()

    barrier = pltpu.get_barrier_semaphore()
    peers = [(f ^ m, t) for m in range(1, nf)] + [(f, t ^ m) for m in range(1, nt)]
    for peer in peers:
        pl.semaphore_signal(barrier, inc=1, device_id=peer, device_id_type=MESH)
    pl.semaphore_wait(barrier, len(peers))

    row_cuts = share_rows(rows, nt)
    col_cuts = nt // row_cuts
    cr, cc = rows // row_cuts, d // col_cuts

    def piece(ref, y, h=None):
        row = pl.multiple_of((y // col_cuts) * cr, cr)
        width = cc if h is None else cc // 2
        col = (y % col_cuts) * cc + (0 if h is None else h * width)
        return ref.at[pl.ds(row, cr), pl.ds(pl.multiple_of(col, width), width)]

    dwh = ff // 2
    lanes = max(subs, 2)
    pah = rows // lanes

    def over_fs(k, source, place, n=2):
        return Gather(nf, f, lambda g: (g, t), source, place, xs.at[k],
                      lambda cls, m: pa_r.at[cls, m - 1] if k == 2 else xr.at[k, cls, m - 1],
                      ("up",) * (n // 2) + ("down",) * (n // 2))

    g_cot = over_fs(0, lambda h: piece(cot_all.at[f], t, h), lambda g, h: piece(cot_all.at[g], t, h))
    g_dw = over_fs(1, lambda h: dw_all.at[pl.ds(h * dwh, dwh), own_cols],
                   lambda g, h: dw_all.at[pl.ds(h * dwh, dwh), pl.ds(pl.multiple_of(g * db, db), db)])
    g_pa = over_fs(2, lambda h: pa_all.at[f, pl.ds(h * pah, pah), :],
                   lambda g, h: pa_all.at[g, pl.ds(h * pah, pah), :], lanes)

    def strip(m, s, y):
        return piece(cot_all.at[f ^ m], y, s if strips == 2 else None)

    def over_z(m, s):
        spot = lambda y, cls=0: strip(m, s, 2 * y + c)
        return Gather(nz, z, lambda y: (f, 2 * y + c), lambda cls: spot(z), spot,
                      zs.at[m - 1, s], lambda cls, k: zr.at[m - 1, s, k - 1], ("down",))

    def to_sibling(m, s, k):
        spot = strip(m, s, 2 * (z ^ k) + c)
        return remote(spot, spot, ss.at[m - 1], sr.at[m - 1], (f, t ^ 1))

    def from_sibling(m):
        spot = cot_all.at[pl.ds(0, nz), pl.ds(0, cr), pl.ds(0, cc)]
        return remote(spot, spot, ss.at[m - 1], sr.at[m - 1], (f, t ^ 1))

    exchange = lambda m: remote(columns(f ^ m, c), in_half(f, c), a_s, a_r.at[m - 1], (f ^ m, t))
    exchanged = lambda m: remote(in_half(f ^ m, c), in_half(f ^ m, c), a_s, a_r.at[m - 1], (f ^ m, t))
    in_to = lambda m: remote(in_half(f ^ m, c), in_half(f ^ m, c), bs, br.at[m - 1], (f, t ^ 1))
    in_from = lambda m: remote(in_half(f ^ m, 1 - c), in_half(f ^ m, 1 - c), bs, br.at[m - 1], (f, t ^ 1))

    masks = by_weight(nf)
    zorder = by_weight(nz, True)
    left = {m: 2 for m in masks}
    rings = {(m, s): over_z(m, s) for m in masks for s in range(strips)}
    singles = [m for m in masks if m & (m - 1) == 0]
    pairs = [(m, cls) for m in masks for cls in (0, 1)]
    inner = [p for p in pairs if g_dw.targets(p[1], p[0])]
    outer = [p for p in pairs if p not in inner]

    def take_cot(items):
        for m, cls in items:
            g_cot.arrive(cls, m)
            g_cot.push(cls, m)
            left[m] -= 1
            if strips == 2:
                rings[m, cls].push(0, 0)
                to_sibling(m, cls, 0).start()
            elif left[m] == 0:
                rings[m, 0].push(0, 0)
                to_sibling(m, 0, 0).start()

    def turn(m, s, steps):
        for k in steps:
            rings[m, s].arrive(0, k)
            rings[m, s].push(0, k)
            to_sibling(m, s, k).start()

    def take(g, items):
        for m, cls in items:
            g.arrive(cls, m)
            g.push(cls, m)

    tile = min(ff, 256)

    def square_grad(m):
        g = f ^ m
        if m:
            from_sibling(m).wait_recv()
        sq[g] = contract_last(cot_all[g], dw_all[...])

    def unit(u):
        m, q, n = u
        g = f ^ m
        i = m * subs + q
        some = pl.ds(q * height, n * height)
        for j in range(ff // tile):
            cols = pl.ds(j * tile, tile)
            active = jnp.maximum(pa_all[g, some, cols].astype(F32), 0.0)
            pre[g, some, cols] = (2.0 * active * sq[g, some, cols]).astype(BF16)
            sqr[g, some, cols] = (active * active).astype(BF16)
        total = contract_last(pre[g, some, :], up_all[...])
        for e in range(n):
            for k in range(nt):
                row, col = ((k % 2) * pr, (k // 2) * pc) if wide else (k * pr, 0)
                row += e * height
                part[k % 2, k // 2, i + e] = total[row:row + pr, col:col + pc]
        halves(u).start()

    wide = height // 2 == pr
    first_slot = lambda u: every.index(u)
    slots = lambda u: pl.ds(u[0] * subs + u[1], u[2])

    def halves(u):
        i = first_slot(u)
        return remote(part.at[1 - c, :, slots(u)], from_sib.at[:, slots(u)], hs.at[i], hr.at[i], (f, t ^ 1))

    def spread(u, k):
        i = first_slot(u)
        return remote(wire.at[k, slots(u)], landed.at[k, slots(u)], ws.at[i], wr.at[i], (f, 2 * (z ^ k) + c))

    def spreads(u):
        i = first_slot(u)
        return remote(wire.at[pl.ds(1, nz - 1), slots(u)], landed.at[pl.ds(1, nz - 1), slots(u)],
                      ws.at[i], wr.at[i], (f, t ^ 2))

    def scatter(u):
        halves(u).wait_recv()
        for k in range(nz - 1, 0, -1):
            wire[k, slots(u)] = (part[c, z ^ k, slots(u)] + from_sib[z ^ k, slots(u)]).astype(BF16)
            spread(u, k).start()

    def home(u, g, k):
        return got.at[g, k, pl.ds(u[1], u[2])]

    def trade(u):
        i = first_slot(u)
        return remote(final.at[slots(u)], home(u, f, t), ts.at[i], tr.at[i], (f ^ u[0], t))

    def traded(u):
        i = first_slot(u)
        spot = home(u, f ^ u[0], t)
        return remote(spot, spot, ts.at[i], tr.at[i], (f ^ u[0], t))

    def finish(u):
        value = part[c, z, slots(u)] + from_sib[z, slots(u)]
        spreads(u).wait()
        for k in range(1, nz):
            value = value + landed[k, slots(u)].astype(F32)
        halves(u).wait_send()
        if u[0] == 0:
            got[f, t, pl.ds(u[1], u[2])] = value.astype(BF16)
        else:
            final[slots(u)] = value.astype(BF16)
            trade(u).start()

    def ring_of(u):
        i = first_slot(u)
        spot = lambda y, cls=0: home(u, f ^ u[0], 2 * y + c)
        return Gather(nz, z, lambda y: (f, 2 * y + c), lambda cls: spot(z), spot,
                      gs.at[i], lambda cls, k: gr.at[i, k - 1],
                      ("flat",) if u in late else ("down",))

    def over(u, k):
        spot = home(u, f ^ u[0], t ^ (2 * k))
        i = first_slot(u)
        return remote(spot, spot, ks.at[i], kr.at[i], (f, t ^ 1))

    def overs(u):
        i = first_slot(u)
        spot = landed.at[:, slots(u)]
        return remote(spot, spot, ks.at[i], kr.at[i], (f, t ^ 1))

    def announce(u):
        if u[0]:
            traded(u).wait_recv()
        outs[u] = ring_of(u)
        outs[u].push(0, 0)
        over(u, 0).start()

    def pass_on(u, steps):
        for k in steps:
            outs[u].arrive(0, k)
            outs[u].push(0, k)
            over(u, k).start()

    def down(m, first):
        g = f ^ m
        value = contract_first(sqr[g], cot_all[g, :, own_cols])
        dgrad[...] = value if first else dgrad[...] + value

    def up_part(m, first):
        g = f ^ m
        value = contract_first(inp_all[g], pre[g])
        ugrad[...] = value if first else ugrad[...] + value

    single = lambda p: p[0] in singles
    near = [p for p in inner if single(p)] + [p for p in outer if single(p)]
    far = [p for p in pairs if not single(p)]
    ahead_k = [k for k in zorder if rings[masks[0], 0].targets(0, k)]
    end_k = [k for k in zorder if k not in ahead_k]
    spots = lambda items: [p for p in items if p[1] < strips]
    near_spots, far_spots = spots(near), spots(far)

    own[0].wait()
    g_cot.push_own()
    own[1].wait()
    g_dw.push_own((0,))
    take_cot(near)
    g_dw.push_own((1,))
    for m, s in near_spots[:2]:
        turn(m, s, ahead_k)
    take(g_dw, inner)
    own[2].wait()
    g_pa.push_own()
    take_cot(far)
    for m, s in near_spots[2:]:
        turn(m, s, ahead_k)
    for m, s in near_spots:
        turn(m, s, end_k)
    for m, s in far_spots:
        turn(m, s, ahead_k)
    take(g_dw, outer)
    for copy in own[3:]:
        copy.wait()

    heads = [(m, q) for j in range(lanes // 2) for q in (j, lanes - 1 - j) for m in masks]
    inner = [p for p in heads if g_pa.targets(p[1], p[0])]
    middle = [p for p in heads if p not in inner and single(p)]
    last = [p for p in heads if p not in inner and not single(p)]
    first_units = [(0, 0, subs)]
    if subs == 1:
        inner_units, middle_units = [], [(m, 0, 1) for m in singles]
        last_units = [(m, 0, 1) for m in masks if m not in singles]
    else:
        side = lanes // 2
        inner_units = [(m, q, side) for m in masks for q in (0, side) if (m, q) in inner]
        middle_units = [(m, q, side) for m in masks for q in (0, side) if (m, q) in middle]
        last_units = [(m, q, 1) for m, q in last]
    early, late = last_units[:len(last_units) // 2], last_units[len(last_units) // 2:]
    outs = {}
    every = first_units + inner_units + middle_units + last_units
    square_grad(0)
    for u in first_units:
        unit(u)
    for m, s in far_spots:
        turn(m, s, end_k)
    square_grad(singles[0])
    for u in first_units:
        scatter(u)
    for m in masks[1:]:
        square_grad(m)

    def come(items):
        for m, cls in items:
            g_pa.arrive(cls, m)

    def forward(items):
        for m, cls in items:
            g_pa.push(cls, m)

    def settle():
        width = cc // strips
        for m in masks:
            from_sibling(m).wait_send()
            for s in range(strips):
                rings[m, s].drain(cot_all.at[pl.ds(0, nz - 1), pl.ds(0, cr), pl.ds(0, width)])
        g_cot.drain(cot_all.at[pl.ds(0, nf - 1), pl.ds(0, cr), pl.ds(0, cc)])
        g_dw.drain(dw_all.at[:, pl.ds(0, (nf - 1) * db)])

    come(inner)
    forward(inner[:len(inner) // 2])
    for u in inner_units:
        unit(u)
    for u in first_units:
        finish(u)
    for u in inner_units:
        scatter(u)
    for u in first_units:
        announce(u)
    settle()
    down(0, True)
    up_part(0, True)
    for u in inner_units:
        finish(u)
    forward(inner[len(inner) // 2:])
    for m in masks:
        if m not in singles:
            exchange(m).start()
    for u in first_units:
        pass_on(u, ahead_k)
    take(g_pa, middle)
    for u in middle_units:
        unit(u)
    for u in middle_units:
        scatter(u)
    for u in first_units:
        pass_on(u, end_k)
    for u in inner_units:
        announce(u)
    for m in singles:
        down(m, False)

    def final_units(items):
        for u in items:
            if subs > 1:
                come([(u[0], u[1])])
            unit(u)
        for u in items:
            scatter(u)

    if subs == 1:
        take(g_pa, last)
    final_units(early)
    for u in middle_units:
        finish(u)
    for m in singles:
        exchange(m).start()
    final_units(late)
    for u in inner_units:
        pass_on(u, ahead_k)
    for u in middle_units:
        announce(u)
    for u in inner_units:
        pass_on(u, end_k)
    for u in early:
        finish(u)
    for m in masks:
        if m not in singles:
            down(m, False)
    for u in late:
        finish(u)
    dn_own[...] = jnp.sum(dgrad[...] * dgrad[...], axis=1).reshape(1, ff)
    downs = [remote(dn_own, dn_all.at[f], ds, dr, (f ^ m, t)) for m in range(1, nf)]
    for copy in downs:
        copy.start()

    def swap_in(items):
        for m in items:
            exchanged(m).wait_recv()
            in_to(m).start()

    swap_in([m for m in masks if m not in singles])
    for u in early:
        announce(u)
    for u in middle_units:
        pass_on(u, ahead_k)
    for u in late:
        announce(u)
    swap_in(singles)
    for m in masks[::-1]:
        in_from(m).wait_recv()
        up_part(m, False)
    un_own[...] = jnp.sum(ugrad[...] * ugrad[...], axis=1).reshape(1, db)
    ups = [remote(un_own, un_all.at[t], us, ur, (f, t ^ m)) for m in range(1, nt)]
    for copy in ups:
        copy.start()
    for u in early:
        pass_on(u, ahead_k)
    for u in middle_units + early:
        pass_on(u, end_k)
    for u in late:
        pass_on(u, zorder)

    def up_sums():
        spot = un_all.at[pl.ds(0, nt - 1)]
        return remote(spot, spot, us, ur, (f, t ^ 1))

    def down_sums():
        spot = dn_all.at[pl.ds(0, nf - 1)]
        return remote(spot, spot, ds, dr, (f ^ 1, t))

    def norms_in():
        dn_all[f] = dn_own[...]
        un_all[t] = un_own[...]
        down_sums().wait_recv()
        up_sums().wait_recv()

    norms_in()

    def gathered():
        for u in every:
            overs(u).wait_recv()

    def drain():
        for u in every:
            outs[u].drain(landed.at[pl.ds(1, nz - 1), slots(u)])
            overs(u).wait_send()
            if u[0]:
                trade(u).wait_send()
        spot = inp_all.at[pl.ds(0, nf - 1), pl.ds(0, ih)]
        remote(spot, spot, a_s, bs, (f, t ^ 1)).wait_send()
        remote(spot, spot, bs, a_s, (f, t ^ 1)).wait_send()
        g_pa.drain(pa_all.at[pl.ds(0, nf - 1)])
        up_sums().wait_send()
        down_sums().wait_send()

    gathered()
    drain()


def fused(nf, nt, cot, dw, pa, inp, up):
    rows, d = inp.shape
    ff, db = dw.shape
    nz = nt // 2
    subs, strips = (4, 2) if nf * nz <= 64 else (1, 1)
    half = rows // subs
    pr, pc = piece_shape(nt, half, db)
    units = nf * subs
    dma = pltpu.SemaphoreType.DMA
    vmem = pl.BlockSpec(memory_space=pltpu.VMEM)
    hbm = pl.BlockSpec(memory_space=pl.ANY)
    V = pltpu.VMEM
    n = nf - 1
    count = 9 if subs == 4 and nf == 4 else nf
    sems = [dma((3,)), dma((2, 2, n)), dma((max(subs, 2), n)), dma((n, strips)), dma((n, strips, nz - 1))]
    sems += [dma((n,)), dma((n,)), dma(()), dma((n,)), dma(()), dma((n,))] + [dma((count,))] * 7
    sems += [dma((count, nz - 1)), dma((count,)), dma((count,)), dma(()), dma(()), dma(()), dma(()), dma((5,))]
    return pl.pallas_call(
        functools.partial(fused_kernel, nf, nt, subs, strips),
        out_shape=[
            V((db, ff), F32), V((ff, db), F32), V((nf, nt, subs, pr, pc), BF16),
            V((nt, 1, db), F32), V((nf, 1, ff), F32),
        ],
        in_specs=[hbm] * 5,
        out_specs=[vmem] * 5,
        scratch_shapes=[
            V((nf, rows, d), BF16), V((ff, d), BF16), V((nf, rows, ff), BF16), V((nf, rows, db), BF16),
            V((db, ff), BF16), V((nf, rows, ff), BF16), V((nf, rows, ff), BF16), V((nf, rows, ff), F32),
            V((2, nz, units, pr, pc), F32), V((nz, units, pr, pc), F32),
            V((nz, units, pr, pc), BF16), V((nz, units, pr, pc), BF16), V((units, pr, pc), BF16),
            V((1, db), F32), V((1, ff), F32),
        ] + sems,
        compiler_params=pltpu.CompilerParams(has_side_effects=True, collective_id=0, vmem_limit_bytes=54 * 2 ** 20),
    )(cot, dw, pa, inp, up)


def deliver_kernel(ugrad, dgrad, got, un_all, dn_all, ug_out, dg_out, out, un_out, dn_out, whole, un_sum, dn_sum, sem):
    nf, nt, subs, pr, pc = got.shape
    rows, d = whole.shape
    half, db = rows // subs, d // nf
    copies = [pltpu.make_async_copy(ugrad, ug_out, sem.at[0]), pltpu.make_async_copy(dgrad, dg_out, sem.at[1])]
    for copy in copies:
        copy.start()
    wide = half // 2 == pr
    for h in range(subs):
        for k in range(nt):
            for g in range(nf):
                row, col = ((k % 2) * pr, (k // 2) * pc) if wide else (k * pr, 0)
                whole[h * half + row:h * half + row + pr, g * db + col:g * db + col + pc] = got[g, k, h]
    un, dn = un_all[0], dn_all[0]
    for k in range(1, nt):
        un = un + un_all[k]
    for k in range(1, nf):
        dn = dn + dn_all[k]
    un_sum[...] = un
    dn_sum[...] = dn
    last = [pltpu.make_async_copy(whole, out, sem.at[2]), pltpu.make_async_copy(un_sum, un_out, sem.at[3]),
            pltpu.make_async_copy(dn_sum, dn_out, sem.at[4])]
    for copy in last:
        copy.start()
    for copy in copies + last:
        copy.wait()


def deliver(rows, d, ugrad, dgrad, got, un_all, dn_all):
    hbm, vmem = pl.BlockSpec(memory_space=pl.ANY), pl.BlockSpec(memory_space=pltpu.VMEM)
    V = pltpu.VMEM
    un, dn = un_all.shape[1:], dn_all.shape[1:]
    H = jax.ShapeDtypeStruct
    return pl.pallas_call(
        deliver_kernel,
        out_shape=[H(ugrad.shape, F32), H(dgrad.shape, F32), H((rows, d), BF16), H(un, F32), H(dn, F32)],
        in_specs=[vmem] * 5,
        out_specs=[hbm] * 5,
        scratch_shapes=[V((rows, d), BF16), V(un, F32), V(dn, F32), pltpu.SemaphoreType.DMA((5,))],
        compiler_params=pltpu.CompilerParams(vmem_limit_bytes=16 * 2 ** 20),
    )(ugrad, dgrad, got, un_all, dn_all)


def local(nf, nt, inputs, pre_act, cotangent, up_weight, down_weight):
    db, ff = up_weight.shape
    parts = fused(nf, nt, cotangent, down_weight, pre_act, inputs, up_weight)
    up_grad, down_grad, out, un, dn = deliver(*inputs.shape, *parts)
    return out, up_grad, down_grad, un.reshape(db), dn.reshape(ff)


def solution(mesh):
    in_specs = (P("fs", None), P("fs", "tp"), P("fs", None), P("fs", "tp"), P("tp", "fs"))
    out_specs = (P("fs", None), P("fs", "tp"), P("tp", "fs"), P("fs"), P("tp"))
    body = functools.partial(local, mesh.shape["fs"], mesh.shape["tp"])
    return jax.shard_map(body, mesh=mesh, in_specs=in_specs, out_specs=out_specs, check_vma=False)
```

```python
import functools

import jax
import jax.numpy as jnp
from jax import lax
from jax.experimental import pallas as pl
from jax.experimental.pallas import tpu as pltpu
from jax.sharding import PartitionSpec as P

MESH = pl.DeviceIdType.MESH
F32, BF16 = jnp.float32, jnp.bfloat16


def contract_last(left, right):
    return lax.dot_general(left, right, (((1,), (1,)), ((), ())), preferred_element_type=F32)


def contract_first(left, right):
    return lax.dot_general(left, right, (((0,), (0,)), ((), ())), preferred_element_type=F32)


def bits_of(n):
    return [1 << i for i in range(n.bit_length() - 1)]


def by_weight(n, down=False):
    return sorted(range(1, n), key=lambda m: (bin(m).count("1"), -m if down else m))


class Gather:
    def __init__(self, n, me, device, source, place, send, recv, orders):
        self.n, self.me, self.device = n, me, device
        self.source, self.place = source, place
        self.send, self.recv, self.orders = send, recv, orders

    def targets(self, cls, m):
        bits = bits_of(self.n)
        if self.orders[cls] == "flat":
            return list(range(self.n - 1, 0, -1)) if m == 0 else []
        if m == 0:
            return bits
        if self.orders[cls] == "up":
            return [b for b in bits if b > m]
        return [b for b in bits if b < (m & -m)]

    def copy(self, cls, m, b):
        there = self.place(self.me ^ m, cls)
        return pltpu.make_async_remote_copy(
            src_ref=self.source(cls) if m == 0 else there,
            dst_ref=there,
            send_sem=self.send,
            recv_sem=self.recv(cls, m ^ b),
            device_id=self.device(self.me ^ b),
            device_id_type=MESH,
        )

    def push(self, cls, m, only=None):
        for b in self.targets(cls, m):
            if only is None or b == only:
                self.copy(cls, m, b).start()

    def push_own(self, turns=None):
        classes = list(range(len(self.orders)))
        for i, b in enumerate(bits_of(self.n)):
            for j, cls in enumerate(classes if i % 2 == 0 else classes[::-1]):
                if turns is None or j in turns:
                    self.push(cls, 0, b)

    def arrive(self, cls, m):
        here = self.place(self.me ^ m, cls)
        pltpu.make_async_remote_copy(
            src_ref=here,
            dst_ref=here,
            send_sem=self.send,
            recv_sem=self.recv(cls, m),
            device_id=self.device(self.me ^ (m & -m)),
            device_id_type=MESH,
        ).wait_recv()

    def drain(self, sent):
        pltpu.make_async_remote_copy(src_ref=sent, dst_ref=sent, send_sem=self.send, recv_sem=self.send,
                                     device_id=self.device(self.me ^ 1), device_id_type=MESH).wait_send()


def share_rows(rows, parts):
    cuts = 1
    while cuts < parts and rows % (2 * cuts * 16) == 0:
        cuts *= 2
    return cuts


def piece_shape(nt, rows, db):
    nz = nt // 2
    if db % (128 * nz) == 0:
        return rows // 2, db // nz
    return rows // nt, db


def fused_kernel(nf, nt, subs, strips, cot, dw, pa, inp, up, ugrad, dgrad, got, un_all, dn_all,
                 cot_own, inp_own, cot_all, dw_all, pa_all, inp_all, up_all, pre, sqr, sq,
                 part, from_sib, wire, landed, final, un_own, dn_own,
                 xs, xr, pa_r, zs, zr, ss, sr, a_s, a_r, bs, br, hs, hr, ws, wr, ts, tr, gs, gr, ks, kr,
                 us, ur, ds, dr, local_sem):
    f, t = lax.axis_index("fs"), lax.axis_index("tp")
    z, c = t // 2, t % 2
    nz = nt // 2
    rows, d = cot.shape
    ff, db = dw.shape
    height = rows // subs
    pr, pc = part.shape[3:]
    own_cols = pl.ds(pl.multiple_of(f * db, db), db)

    def remote(src, dst, send, recv, device):
        return pltpu.make_async_remote_copy(src_ref=src, dst_ref=dst, send_sem=send, recv_sem=recv,
                                            device_id=device, device_id_type=MESH)

    ih = rows // 2

    def columns(g, side):
        return inp.at[pl.ds(pl.multiple_of(side * ih, ih), ih), pl.ds(pl.multiple_of(g * db, db), db)]

    def in_half(g, side):
        return inp_all.at[g, pl.ds(pl.multiple_of(side * ih, ih), ih), :]

    row_cuts = share_rows(rows, nt)
    col_cuts = nt // row_cuts
    cr, cc = rows // row_cuts, d // col_cuts
    first_piece = cot.at[pl.ds(pl.multiple_of((t // col_cuts) * cr, cr), cr),
                         pl.ds(pl.multiple_of((t % col_cuts) * cc, cc), cc)]
    own = [
        pltpu.make_async_copy(first_piece, cot_own, local_sem.at[0]),
        pltpu.make_async_copy(dw, dw_all.at[:, own_cols], local_sem.at[1]),
        pltpu.make_async_copy(pa, pa_all.at[f], local_sem.at[2]),
        pltpu.make_async_copy(cot, cot_all.at[f], local_sem.at[3]),
        pltpu.make_async_copy(up, up_all, local_sem.at[4]),
        pltpu.make_async_copy(inp.at[:, own_cols], inp_all.at[f], local_sem.at[5]),
        pltpu.make_async_copy(inp, inp_own, local_sem.at[6]),
    ]
    for copy in own[:2]:
        copy.start()

    barrier = pltpu.get_barrier_semaphore()
    peers = [(f ^ m, t) for m in range(1, nf)] + [(f, t ^ m) for m in range(1, nt)]
    for peer in peers:
        pl.semaphore_signal(barrier, inc=1, device_id=peer, device_id_type=MESH)
    pl.semaphore_wait(barrier, len(peers))

    def piece(ref, y, h=None):
        row = pl.multiple_of((y // col_cuts) * cr, cr)
        width = cc if h is None else cc // 2
        col = (y % col_cuts) * cc + (0 if h is None else h * width)
        return ref.at[pl.ds(row, cr), pl.ds(pl.multiple_of(col, width), width)]

    dwh = ff // 2
    lanes = max(subs, 2)
    pah = rows // lanes

    def over_fs(k, source, place, n=2):
        return Gather(nf, f, lambda g: (g, t), source, place, xs.at[k],
                      lambda cls, m: pa_r.at[cls, m - 1] if k == 2 else xr.at[k, cls, m - 1],
                      ("up",) * (n // 2) + ("down",) * (n // 2))

    g_cot = over_fs(0, lambda h: cot_own.at[:, pl.ds(h * (cc // 2), cc // 2)], lambda g, h: piece(cot_all.at[g], t, h))
    g_dw = over_fs(1, lambda h: dw_all.at[pl.ds(h * dwh, dwh), own_cols],
                   lambda g, h: dw_all.at[pl.ds(h * dwh, dwh), pl.ds(pl.multiple_of(g * db, db), db)])
    g_pa = over_fs(2, lambda h: pa_all.at[f, pl.ds(h * pah, pah), :],
                   lambda g, h: pa_all.at[g, pl.ds(h * pah, pah), :], lanes)

    def strip(m, s, y):
        return piece(cot_all.at[f ^ m], y, s if strips == 2 else None)

    def over_z(m, s):
        spot = lambda y, cls=0: strip(m, s, 2 * y + c)
        return Gather(nz, z, lambda y: (f, 2 * y + c), lambda cls: spot(z), spot,
                      zs.at[m - 1, s], lambda cls, k: zr.at[m - 1, s, k - 1], ("down",))

    def to_sibling(m, s, k):
        spot = strip(m, s, 2 * (z ^ k) + c)
        return remote(spot, spot, ss.at[m - 1], sr.at[m - 1], (f, t ^ 1))

    def from_sibling(m):
        spot = cot_all.at[pl.ds(0, nz), pl.ds(0, cr), pl.ds(0, cc)]
        return remote(spot, spot, ss.at[m - 1], sr.at[m - 1], (f, t ^ 1))

    iq = rows // 4
    seat = lambda y: (2 * y + c)

    def quarter(g, q):
        return inp_all.at[g, pl.ds(pl.multiple_of(q * iq, iq), iq), :]

    def source(m):
        height, q = (iq, seat(z % 2)) if m == deep_m else (ih, c)
        return inp_own.at[pl.ds(pl.multiple_of(q * height, height), height), pl.ds(pl.multiple_of((f ^ m) * db, db), db)]

    def place(m, g):
        return quarter(g, seat(z % 2)) if m == deep_m else in_half(g, c)

    exchange = lambda m: remote(source(m), place(m, f), a_s.at[m - 1], a_r.at[m - 1], (f ^ m, t))
    exchanged = lambda m: remote(place(m, f ^ m), place(m, f ^ m), a_s.at[m - 1], a_r.at[m - 1], (f ^ m, t))
    in_to = lambda m: remote(place(m, f ^ m), place(m, f ^ m), bs.at[m - 1], br.at[m - 1], (f, t ^ 1))

    def in_from(m):
        return remote(in_half(f ^ m, 1 - c), in_half(f ^ m, 1 - c), bs.at[m - 1], br.at[m - 1], (f, t ^ 1))

    def in_z():
        spot = quarter(f ^ deep_m, seat(z % 2))
        return remote(spot, spot, a_s.at[nf - 1], a_r.at[nf - 1], (f, t ^ 2))

    def in_z_from():
        spot = quarter(f ^ deep_m, seat(1 - z % 2))
        return remote(spot, spot, a_s.at[nf - 1], a_r.at[nf - 1], (f, t ^ 2))

    def in_to_z():
        spot = quarter(f ^ deep_m, seat(1 - z % 2))
        return remote(spot, spot, bs.at[deep_m - 1], br.at[deep_m - 1], (f, t ^ 1))

    masks = by_weight(nf)
    deep_m = masks[-1]
    zorder = by_weight(nz, True)
    left = {m: 2 for m in masks}
    rings = {(m, s): over_z(m, s) for m in masks for s in range(strips)}
    singles = [m for m in masks if m & (m - 1) == 0]
    pairs = [(m, cls) for m in masks for cls in (0, 1)]
    inner = [p for p in pairs if g_dw.targets(p[1], p[0])]
    outer = [p for p in pairs if p not in inner]

    def take_cot(items):
        for m, cls in items:
            g_cot.arrive(cls, m)
            g_cot.push(cls, m)
            left[m] -= 1
            if strips == 2:
                rings[m, cls].push(0, 0)
                to_sibling(m, cls, 0).start()
            elif left[m] == 0:
                rings[m, 0].push(0, 0)
                to_sibling(m, 0, 0).start()

    def turn(m, s, steps):
        for k in steps:
            rings[m, s].arrive(0, k)
            rings[m, s].push(0, k)
            to_sibling(m, s, k).start()

    def take(g, items):
        for m, cls in items:
            g.arrive(cls, m)
            g.push(cls, m)

    tile = min(ff, 256)

    def term(m, k):
        cols = pl.ds(pl.multiple_of((f ^ k) * db, db), db)
        return contract_last(cot_all[f ^ m, :, cols], dw_all[:, cols])

    def square_start(m):
        if m:
            from_sibling(m).wait_recv()
        total = term(m, 0)
        for k in masks[:-1]:
            total = total + term(m, k)
        sq[f ^ m] = total

    def square_end(m):
        sq[f ^ m] += term(m, masks[-1])

    def unit(u):
        m, q, n = u
        g = f ^ m
        i = m * subs + q
        some = pl.ds(q * height, n * height)
        for j in range(ff // tile):
            cols = pl.ds(j * tile, tile)
            active = jnp.maximum(pa_all[g, some, cols].astype(F32), 0.0)
            pre[g, some, cols] = (2.0 * active * sq[g, some, cols]).astype(BF16)
            sqr[g, some, cols] = (active * active).astype(BF16)
        total = contract_last(pre[g, some, :], up_all[...])
        for e in range(n):
            for k in range(nt):
                row, col = ((k % 2) * pr, (k // 2) * pc) if wide else (k * pr, 0)
                row += e * height
                part[k % 2, k // 2, i + e] = total[row:row + pr, col:col + pc]
        halves(u).start()

    wide = height // 2 == pr
    first_slot = lambda u: every.index(u)
    slots = lambda u: pl.ds(u[0] * subs + u[1], u[2])

    def halves(u):
        i = first_slot(u)
        return remote(part.at[1 - c, :, slots(u)], from_sib.at[:, slots(u)], hs, hr.at[i], (f, t ^ 1))

    def spread(u, k):
        i = first_slot(u)
        return remote(wire.at[k, slots(u)], landed.at[k, slots(u)], ws, wr.at[i], (f, 2 * (z ^ k) + c))

    def spreads(u):
        i = first_slot(u)
        return remote(wire.at[pl.ds(1, nz - 1), slots(u)], landed.at[pl.ds(1, nz - 1), slots(u)],
                      ws, wr.at[i], (f, t ^ 2))

    def scatter(u):
        halves(u).wait_recv()
        for k in range(nz - 1, 0, -1):
            wire[k, slots(u)] = (part[c, z ^ k, slots(u)] + from_sib[z ^ k, slots(u)]).astype(BF16)
            spread(u, k).start()

    def home(u, g, k):
        return got.at[g, k, pl.ds(u[1], u[2])]

    def trade(u):
        i = first_slot(u)
        return remote(final.at[slots(u)], home(u, f, t), ts, tr.at[i], (f ^ u[0], t))

    def traded(u):
        i = first_slot(u)
        spot = home(u, f ^ u[0], t)
        return remote(spot, spot, ts, tr.at[i], (f ^ u[0], t))

    def finish(u):
        value = part[c, z, slots(u)] + from_sib[z, slots(u)]
        spreads(u).wait_recv()
        for k in range(1, nz):
            value = value + landed[k, slots(u)].astype(F32)
        if u[0] == 0:
            got[f, t, pl.ds(u[1], u[2])] = value.astype(BF16)
        else:
            final[slots(u)] = value.astype(BF16)
            trade(u).start()

    def ring_of(u):
        i = first_slot(u)
        spot = lambda y, cls=0: home(u, f ^ u[0], 2 * y + c)
        return Gather(nz, z, lambda y: (f, 2 * y + c), lambda cls: spot(z), spot,
                      gs, lambda cls, k: gr.at[i, k - 1],
                      ("flat",) if u in flats else ("down",))

    def over(u, k):
        spot = home(u, f ^ u[0], t ^ (2 * k))
        return remote(spot, spot, ks, kr, (f, t ^ 1))

    def announce(u):
        if u[0]:
            traded(u).wait_recv()
        outs[u] = ring_of(u)
        outs[u].push(0, 0)
        over(u, 0).start()

    def pass_on(u, steps):
        for k in steps:
            outs[u].arrive(0, k)
            outs[u].push(0, k)
            over(u, k).start()

    def down(m, first):
        g = f ^ m
        value = contract_first(sqr[g], cot_all[g, :, own_cols])
        dgrad[...] = value if first else dgrad[...] + value

    def up_part(m, first):
        g = f ^ m
        value = contract_first(inp_all[g], pre[g])
        ugrad[...] = value if first else ugrad[...] + value

    single = lambda p: p[0] in singles
    near = [p for p in inner if single(p)] + [p for p in outer if single(p)]
    far = [p for p in pairs if not single(p)]
    ahead_k = [k for k in zorder if rings[masks[0], 0].targets(0, k)]
    end_k = [k for k in zorder if k not in ahead_k]
    spots = lambda items: [p for p in items if p[1] < strips]
    near_spots, far_spots = spots(near), spots(far)

    own[0].wait()
    g_cot.push_own()
    own[1].wait()
    g_dw.push_own((0,))
    for copy in own[2:]:
        copy.start()
    take_cot(near)
    g_dw.push_own((1,))
    for m, s in near_spots[:2]:
        turn(m, s, ahead_k)
    take(g_dw, inner)
    own[2].wait()
    g_pa.push_own((0, 1))
    take_cot(far)
    for m, s in near_spots[2:]:
        turn(m, s, ahead_k)
    for m, s in near_spots:
        turn(m, s, end_k)
    for m, s in far_spots:
        turn(m, s, ahead_k)
    take(g_dw, [p for p in outer if p[0] != masks[-1]])
    own[3].wait()
    for m in [0] + singles:
        square_start(m)
    take(g_dw, [p for p in outer if p[0] == masks[-1]])
    for copy in own[4:]:
        copy.wait()

    first = (0, 0, subs)
    if subs == 1:
        steps = [[(m, 0, 1)] for m in masks]
    else:
        side = lanes // 2
        ends = lambda items, j: [(m, q, 1) for m, q in items if q in (j, lanes - 1 - j)]
        heads = [(m, q) for m in masks for q in range(lanes)]
        lead = [p for p in heads if g_pa.targets(p[1], p[0])]
        tail = [p for p in heads if p not in lead and p[0] in singles]
        deep = [p for p in heads if p not in lead and p[0] not in singles]
        steps = [ends(lead, j) for j in range(side)] + [ends(deep, j) for j in range(side)]
        steps += [[(m, q, 1) for m, q in tail if q in ((j, lanes - 1 - j) if m == singles[-1] else (lanes - 1 - j, j))]
                  for j in range(side - 1, -1, -1)]
    every = [first] + [u for items in steps for u in items]
    count = len(steps)
    flats = [u for items in steps[-2:] for u in items]
    outs = {}

    def come(items):
        for m, q, n in items:
            g_pa.arrive(q, m)

    def forward(items):
        for m, q, n in items:
            g_pa.push(q, m)

    def settle():
        width = cc // strips
        for m in masks:
            from_sibling(m).wait_send()
            for s in range(strips):
                rings[m, s].drain(cot_all.at[pl.ds(0, nz - 1), pl.ds(0, cr), pl.ds(0, width)])
        g_cot.drain(cot_all.at[pl.ds(0, nf - 1), pl.ds(0, cr), pl.ds(0, cc)])
        g_dw.drain(dw_all.at[:, pl.ds(0, (nf - 1) * db)])

    def swap_in(items):
        for m in items:
            exchanged(m).wait_recv()
            in_to(m).start()
            if m == deep_m:
                in_z().start()

    def fill(j):
        for job in jobs.pop(j, []):
            job()

    def refill(j):
        if subs == 1:
            if j == 0:
                for m in masks:
                    exchange(m).start()
            return
        if j < side:
            forward(steps[j])
        elif j < lanes:
            g_pa.push_own((j,))
        elif j == lanes:
            exchange(deep_m).start()
        else:
            for m in masks[:-1]:
                exchange(m).start()

    groups = lambda i: [first] if i < 0 else steps[i]

    def run(i):
        if subs > 1:
            come(steps[i])
        refill(i)
        for u in steps[i]:
            unit(u)
        if 2 <= i < count - 1:
            for u in groups(i - 3):
                announce(u)
        fill(i)
        for u in steps[i]:
            scatter(u)
        if i >= 2 and i == count - 1:
            for u in groups(i - 3):
                announce(u)
        if i == 1:
            finish(first)
        for u in steps[i - 1] if i else []:
            finish(u)
        if i >= 3:
            for u in groups(i - 4):
                pass_on(u, near_k(u))

    near_k = lambda u: [] if u in flats else ahead_k
    rest_k = lambda u: outs[u].targets(0, 0) if u in flats else end_k
    jobs = {
        0: [lambda: square_start(masks[-1]), lambda: square_end(masks[-1])] if subs > 1 else [],
        1: [settle],
        2: [lambda: down(0, True)],
        3: [lambda: up_part(0, True)],
        4: [lambda: down(masks[-1], False)],
    }

    square_end(0)
    unit(first)
    for m in singles:
        square_end(m)
    for m, s in far_spots:
        turn(m, s, end_k)
    if subs == 1:
        for m in masks:
            if m not in singles:
                square_start(m)
                square_end(m)
        for cls in range(lanes):
            for m in masks:
                g_pa.arrive(cls, m)
                g_pa.push(cls, m)
    scatter(first)
    for i in range(count):
        run(i)
    for j in sorted(jobs):
        fill(j)
    swap_in(masks[-1:])
    for u in steps[-3]:
        announce(u)
    for m in masks if subs == 1 else singles:
        if not (subs == 1 and m == masks[-1]):
            down(m, False)
    for u in steps[-1]:
        finish(u)
    for u in steps[-4]:
        pass_on(u, near_k(u))
    for u in steps[-2]:
        announce(u)
    dn_own[...] = jnp.sum(dgrad[...] * dgrad[...], axis=1).reshape(1, ff)
    downs = [remote(dn_own, dn_all.at[f], ds, dr, (f ^ m, t)) for m in range(1, nf)]
    for copy in downs:
        copy.start()
    swap_in(masks[:-1])
    for u in steps[-3]:
        pass_on(u, near_k(u))
    for u in steps[-1]:
        announce(u)
    in_z_from().wait_recv()
    in_to_z().start()
    for m in masks:
        in_from(m).wait_recv()
        up_part(m, False)
    un_own[...] = jnp.sum(ugrad[...] * ugrad[...], axis=1).reshape(1, db)
    ups = [remote(un_own, un_all.at[t], us, ur, (f, t ^ m)) for m in range(1, nt)]
    for copy in ups:
        copy.start()
    for u in [first] + [u for items in steps for u in items]:
        pass_on(u, rest_k(u))

    def up_sums():
        spot = un_all.at[pl.ds(0, nt - 1)]
        return remote(spot, spot, us, ur, (f, t ^ 1))

    def down_sums():
        spot = dn_all.at[pl.ds(0, nf - 1)]
        return remote(spot, spot, ds, dr, (f ^ 1, t))

    def norms_in():
        dn_all[f] = dn_own[...]
        un_all[t] = un_own[...]
        down_sums().wait_recv()
        up_sums().wait_recv()

    norms_in()

    def gathered():
        remote(landed, landed, ks, kr, (f, t ^ 1)).wait_recv()

    def drain():
        most = landed.at[pl.ds(1, nz - 1)]
        remote(landed, landed, ks, kr, (f, t ^ 1)).wait_send()
        remote(most, most, ws, kr, (f, t ^ 2)).wait_send()
        remote(most, most, gs, kr, (f, t ^ 2)).wait_send()
        remote(from_sib, from_sib, hs, kr, (f, t ^ 1)).wait_send()
        traded_all = final.at[pl.ds(subs, (nf - 1) * subs)]
        remote(traded_all, traded_all, ts, kr, (f ^ 1, t)).wait_send()
        for m in masks:
            exchange(m).wait_send()
            in_from(m).wait_send()
        in_z().wait_send()
        g_pa.drain(pa_all.at[pl.ds(0, nf - 1)])
        up_sums().wait_send()
        down_sums().wait_send()

    gathered()
    drain()


def fused(nf, nt, cot, dw, pa, inp, up):
    rows, d = inp.shape
    ff, db = dw.shape
    nz = nt // 2
    subs, strips = (4, 2) if nf * nz <= 64 else (1, 1)
    half = rows // subs
    pr, pc = piece_shape(nt, half, db)
    units = nf * subs
    dma = pltpu.SemaphoreType.DMA
    vmem = pl.BlockSpec(memory_space=pltpu.VMEM)
    hbm = pl.BlockSpec(memory_space=pl.ANY)
    V = pltpu.VMEM
    n = nf - 1
    cuts = share_rows(rows, nt)
    count = 1 + n * subs
    sems = [dma((3,)), dma((2, 2, n)), dma((max(subs, 2), n)), dma((n, strips)), dma((n, strips, nz - 1))]
    sems += [dma((n,)), dma((n,)), dma((nf,)), dma((nf,)), dma((n,)), dma((n,))]
    sems += [dma(()), dma((count,)), dma(()), dma((count,)), dma(()), dma((count,)), dma(()), dma((count, nz - 1))]
    sems += [dma(())] * 6 + [dma((7,))]
    return pl.pallas_call(
        functools.partial(fused_kernel, nf, nt, subs, strips),
        out_shape=[
            V((db, ff), F32), V((ff, db), F32), V((nf, nt, subs, pr, pc), BF16),
            V((nt, 1, db), F32), V((nf, 1, ff), F32),
        ],
        in_specs=[hbm] * 5,
        out_specs=[vmem] * 5,
        scratch_shapes=[
            V((rows // cuts, d * cuts // nt), BF16), V((rows, d), BF16),
            V((nf, rows, d), BF16), V((ff, d), BF16), V((nf, rows, ff), BF16), V((nf, rows, db), BF16),
            V((db, ff), BF16), V((nf, rows, ff), BF16), V((nf, rows, ff), BF16), V((nf, rows, ff), F32),
            V((2, nz, units, pr, pc), F32), V((nz, units, pr, pc), F32),
            V((nz, units, pr, pc), BF16), V((nz, units, pr, pc), BF16), V((units, pr, pc), BF16),
            V((1, db), F32), V((1, ff), F32),
        ] + sems,
        compiler_params=pltpu.CompilerParams(has_side_effects=True, collective_id=0, vmem_limit_bytes=54 * 2 ** 20),
    )(cot, dw, pa, inp, up)


def deliver_kernel(ugrad, dgrad, got, un_all, dn_all, ug_out, dg_out, out, un_out, dn_out, whole, un_sum, dn_sum, sem):
    nf, nt, subs, pr, pc = got.shape
    rows, d = whole.shape
    half, db = rows // subs, d // nf
    copies = [pltpu.make_async_copy(ugrad, ug_out, sem.at[0]), pltpu.make_async_copy(dgrad, dg_out, sem.at[1])]
    for copy in copies:
        copy.start()
    wide = half // 2 == pr
    for h in range(subs):
        for k in range(nt):
            for g in range(nf):
                row, col = ((k % 2) * pr, (k // 2) * pc) if wide else (k * pr, 0)
                whole[h * half + row:h * half + row + pr, g * db + col:g * db + col + pc] = got[g, k, h]
    un, dn = un_all[0], dn_all[0]
    for k in range(1, nt):
        un = un + un_all[k]
    for k in range(1, nf):
        dn = dn + dn_all[k]
    un_sum[...] = un
    dn_sum[...] = dn
    last = [pltpu.make_async_copy(whole, out, sem.at[2]), pltpu.make_async_copy(un_sum, un_out, sem.at[3]),
            pltpu.make_async_copy(dn_sum, dn_out, sem.at[4])]
    for copy in last:
        copy.start()
    for copy in copies + last:
        copy.wait()


def deliver(rows, d, ugrad, dgrad, got, un_all, dn_all):
    hbm, vmem = pl.BlockSpec(memory_space=pl.ANY), pl.BlockSpec(memory_space=pltpu.VMEM)
    V = pltpu.VMEM
    un, dn = un_all.shape[1:], dn_all.shape[1:]
    H = jax.ShapeDtypeStruct
    return pl.pallas_call(
        deliver_kernel,
        out_shape=[H(ugrad.shape, F32), H(dgrad.shape, F32), H((rows, d), BF16), H(un, F32), H(dn, F32)],
        in_specs=[vmem] * 5,
        out_specs=[hbm] * 5,
        scratch_shapes=[V((rows, d), BF16), V(un, F32), V(dn, F32), pltpu.SemaphoreType.DMA((5,))],
        compiler_params=pltpu.CompilerParams(vmem_limit_bytes=16 * 2 ** 20),
    )(ugrad, dgrad, got, un_all, dn_all)


def local(nf, nt, inputs, pre_act, cotangent, up_weight, down_weight):
    db, ff = up_weight.shape
    parts = fused(nf, nt, cotangent, down_weight, pre_act, inputs, up_weight)
    up_grad, down_grad, out, un, dn = deliver(*inputs.shape, *parts)
    return out, up_grad, down_grad, un.reshape(db), dn.reshape(ff)


def solution(mesh):
    in_specs = (P("fs", None), P("fs", "tp"), P("fs", None), P("fs", "tp"), P("tp", "fs"))
    out_specs = (P("fs", None), P("fs", "tp"), P("tp", "fs"), P("fs"), P("tp"))
    body = functools.partial(local, mesh.shape["fs"], mesh.shape["tp"])
    return jax.shard_map(body, mesh=mesh, in_specs=in_specs, out_specs=out_specs, check_vma=False)
```

```python
import functools

import jax
import jax.numpy as jnp
from jax import lax
from jax.experimental import pallas as pl
from jax.experimental.pallas import tpu as pltpu
from jax.sharding import PartitionSpec as P

MESH = pl.DeviceIdType.MESH
F32, BF16 = jnp.float32, jnp.bfloat16


def contract_last(left, right):
    return lax.dot_general(left, right, (((1,), (1,)), ((), ())), preferred_element_type=F32)


def contract_first(left, right):
    return lax.dot_general(left, right, (((0,), (0,)), ((), ())), preferred_element_type=F32)


def bits_of(n):
    return [1 << i for i in range(n.bit_length() - 1)]


def by_weight(n, down=False):
    return sorted(range(1, n), key=lambda m: (bin(m).count("1"), -m if down else m))


class Gather:
    def __init__(self, n, me, device, source, place, send, recv, orders):
        self.n, self.me, self.device = n, me, device
        self.source, self.place = source, place
        self.send, self.recv, self.orders = send, recv, orders

    def targets(self, cls, m):
        bits = bits_of(self.n)
        if self.orders[cls] == "flat":
            return list(range(self.n - 1, 0, -1)) if m == 0 else []
        if m == 0:
            return bits
        if self.orders[cls] == "up":
            return [b for b in bits if b > m]
        return [b for b in bits if b < (m & -m)]

    def copy(self, cls, m, b):
        there = self.place(self.me ^ m, cls)
        return pltpu.make_async_remote_copy(
            src_ref=self.source(cls) if m == 0 else there,
            dst_ref=there,
            send_sem=self.send,
            recv_sem=self.recv(cls, m ^ b),
            device_id=self.device(self.me ^ b),
            device_id_type=MESH,
        )

    def push(self, cls, m, only=None):
        for b in self.targets(cls, m):
            if only is None or b == only:
                self.copy(cls, m, b).start()

    def push_own(self, turns=None):
        classes = list(range(len(self.orders)))
        for i, b in enumerate(bits_of(self.n)):
            for j, cls in enumerate(classes if i % 2 == 0 else classes[::-1]):
                if turns is None or j in turns:
                    self.push(cls, 0, b)

    def arrive(self, cls, m):
        here = self.place(self.me ^ m, cls)
        pltpu.make_async_remote_copy(
            src_ref=here,
            dst_ref=here,
            send_sem=self.send,
            recv_sem=self.recv(cls, m),
            device_id=self.device(self.me ^ (m & -m)),
            device_id_type=MESH,
        ).wait_recv()

    def drain(self, sent):
        pltpu.make_async_remote_copy(src_ref=sent, dst_ref=sent, send_sem=self.send, recv_sem=self.send,
                                     device_id=self.device(self.me ^ 1), device_id_type=MESH).wait_send()


def share_rows(rows, parts):
    cuts = 1
    while cuts < parts and rows % (2 * cuts * 16) == 0:
        cuts *= 2
    return cuts


def piece_shape(nt, rows, db):
    nz = nt // 2
    if db % (128 * nz) == 0:
        return rows // 2, db // nz
    return rows // nt, db


def fused_kernel(nf, nt, subs, strips, cot, dw, pa, inp, up, ugrad, dgrad, got, un_all, dn_all,
                 cot_own, inp_own, cot_all, dw_all, pa_all, inp_all, up_all, pre, sqr, sq,
                 part, from_sib, wire, landed, final, un_own, dn_own,
                 xs, xr, pa_r, zs, zr, ss, sr, a_s, a_r, bs, br, hs, hr, ws, wr, ts, tr, gs, gr, ks, kr,
                 us, ur, ds, dr, local_sem):
    f, t = lax.axis_index("fs"), lax.axis_index("tp")
    z, c = t // 2, t % 2
    nz = nt // 2
    rows, d = cot.shape
    ff, db = dw.shape
    height = rows // subs
    pr, pc = part.shape[3:]
    own_cols = pl.ds(pl.multiple_of(f * db, db), db)

    def remote(src, dst, send, recv, device):
        return pltpu.make_async_remote_copy(src_ref=src, dst_ref=dst, send_sem=send, recv_sem=recv,
                                            device_id=device, device_id_type=MESH)

    ih = rows // 2

    def columns(g, side):
        return inp.at[pl.ds(pl.multiple_of(side * ih, ih), ih), pl.ds(pl.multiple_of(g * db, db), db)]

    def in_half(g, side):
        return inp_all.at[g, pl.ds(pl.multiple_of(side * ih, ih), ih), :]

    row_cuts = share_rows(rows, nt)
    col_cuts = nt // row_cuts
    cr, cc = rows // row_cuts, d // col_cuts
    first_piece = cot.at[pl.ds(pl.multiple_of((t // col_cuts) * cr, cr), cr),
                         pl.ds(pl.multiple_of((t % col_cuts) * cc, cc), cc)]
    own = [
        pltpu.make_async_copy(first_piece, cot_own, local_sem.at[0]),
        pltpu.make_async_copy(dw, dw_all.at[:, own_cols], local_sem.at[1]),
        pltpu.make_async_copy(pa, pa_all.at[f], local_sem.at[2]),
        pltpu.make_async_copy(cot, cot_all.at[f], local_sem.at[3]),
        pltpu.make_async_copy(up, up_all, local_sem.at[4]),
        pltpu.make_async_copy(inp.at[:, own_cols], inp_all.at[f], local_sem.at[5]),
        pltpu.make_async_copy(inp, inp_own, local_sem.at[6]),
    ]
    for copy in own[:2]:
        copy.start()

    barrier = pltpu.get_barrier_semaphore()
    peers = [(f ^ m, t) for m in range(1, nf)] + [(f, t ^ m) for m in range(1, nt)]
    for peer in peers:
        pl.semaphore_signal(barrier, inc=1, device_id=peer, device_id_type=MESH)
    pl.semaphore_wait(barrier, len(peers))

    def piece(ref, y, h=None):
        row = pl.multiple_of((y // col_cuts) * cr, cr)
        width = cc if h is None else cc // 2
        col = (y % col_cuts) * cc + (0 if h is None else h * width)
        return ref.at[pl.ds(row, cr), pl.ds(pl.multiple_of(col, width), width)]

    dwh = ff // 2
    lanes = max(subs, 2)
    pah = rows // lanes

    def pa_turn(cls, m):
        return cls * (nf - 1) + m - 1 if subs == 1 else turns[m, cls, 1] - 1

    def over_fs(k, source, place, n=2):
        return Gather(nf, f, lambda g: (g, t), source, place, xs.at[k],
                      lambda cls, m: pa_r.at[pa_turn(cls, m)] if k == 2 else xr.at[k, cls, m - 1],
                      ("up",) * (n // 2) + ("down",) * (n // 2))

    g_cot = over_fs(0, lambda h: cot_own.at[:, pl.ds(h * (cc // 2), cc // 2)], lambda g, h: piece(cot_all.at[g], t, h))
    g_dw = over_fs(1, lambda h: dw_all.at[pl.ds(h * dwh, dwh), own_cols],
                   lambda g, h: dw_all.at[pl.ds(h * dwh, dwh), pl.ds(pl.multiple_of(g * db, db), db)])
    g_pa = over_fs(2, lambda h: pa_all.at[f, pl.ds(h * pah, pah), :],
                   lambda g, h: pa_all.at[g, pl.ds(h * pah, pah), :], lanes)

    def strip(m, s, y):
        return piece(cot_all.at[f ^ m], y, s if strips == 2 else None)

    def over_z(m, s):
        spot = lambda y, cls=0: strip(m, s, 2 * y + c)
        return Gather(nz, z, lambda y: (f, 2 * y + c), lambda cls: spot(z), spot,
                      zs.at[m - 1, s], lambda cls, k: zr.at[m - 1, s, k - 1], ("down",))

    def to_sibling(m, s, k):
        spot = strip(m, s, 2 * (z ^ k) + c)
        return remote(spot, spot, ss.at[m - 1], sr.at[m - 1], (f, t ^ 1))

    def from_sibling(m):
        spot = cot_all.at[pl.ds(0, nz), pl.ds(0, cr), pl.ds(0, cc)]
        return remote(spot, spot, ss.at[m - 1], sr.at[m - 1], (f, t ^ 1))

    iq = rows // 4
    seat = lambda y: (2 * y + c)

    def quarter(g, q):
        return inp_all.at[g, pl.ds(pl.multiple_of(q * iq, iq), iq), :]

    def source(m):
        height, q = (iq, seat(z % 2)) if m == deep_m else (ih, c)
        return inp_own.at[pl.ds(pl.multiple_of(q * height, height), height), pl.ds(pl.multiple_of((f ^ m) * db, db), db)]

    def place(m, g):
        return quarter(g, seat(z % 2)) if m == deep_m else in_half(g, c)

    def exchange(m, part=None):
        src, dst = source(m), place(m, f)
        if part is not None:
            src, dst = src.at[pl.ds(part * iq, iq)], dst.at[pl.ds(part * iq, iq)]
        return remote(src, dst, a_s.at[m - 1], a_r.at[m - 1], (f ^ m, t))

    exchanged = lambda m: remote(place(m, f ^ m), place(m, f ^ m), a_s.at[m - 1], a_r.at[m - 1], (f ^ m, t))
    in_to = lambda m: remote(place(m, f ^ m), place(m, f ^ m), bs.at[m - 1], br.at[m - 1], (f, t ^ 1))

    def in_from(m):
        return remote(in_half(f ^ m, 1 - c), in_half(f ^ m, 1 - c), bs.at[m - 1], br.at[m - 1], (f, t ^ 1))

    def in_z():
        spot = quarter(f ^ deep_m, seat(z % 2))
        return remote(spot, spot, a_s.at[nf - 1], a_r.at[nf - 1], (f, t ^ 2))

    def in_z_from():
        spot = quarter(f ^ deep_m, seat(1 - z % 2))
        return remote(spot, spot, a_s.at[nf - 1], a_r.at[nf - 1], (f, t ^ 2))

    def in_to_z():
        spot = quarter(f ^ deep_m, seat(1 - z % 2))
        return remote(spot, spot, bs.at[deep_m - 1], br.at[deep_m - 1], (f, t ^ 1))

    masks = by_weight(nf)
    deep_m = masks[-1]
    zorder = by_weight(nz, True)
    left = {m: 2 for m in masks}
    rings = {(m, s): over_z(m, s) for m in masks for s in range(strips)}
    singles = [m for m in masks if m & (m - 1) == 0]
    pairs = [(m, cls) for m in masks for cls in (0, 1)]
    inner = [p for p in pairs if g_dw.targets(p[1], p[0])]
    outer = [p for p in pairs if p not in inner]

    def take_cot(items):
        for m, cls in items:
            g_cot.arrive(cls, m)
            g_cot.push(cls, m)
            left[m] -= 1
            if strips == 2:
                rings[m, cls].push(0, 0)
                to_sibling(m, cls, 0).start()
            elif left[m] == 0:
                rings[m, 0].push(0, 0)
                to_sibling(m, 0, 0).start()

    def turn(m, s, steps):
        for k in steps:
            rings[m, s].arrive(0, k)
            rings[m, s].push(0, k)
            to_sibling(m, s, k).start()

    def take(g, items):
        for m, cls in items:
            g.arrive(cls, m)
            g.push(cls, m)

    tile = min(ff, 256)

    def term(m, k):
        cols = pl.ds(pl.multiple_of((f ^ k) * db, db), db)
        return contract_last(cot_all[f ^ m, :, cols], dw_all[:, cols])

    def square_start(m):
        if m:
            from_sibling(m).wait_recv()
        total = term(m, 0)
        for k in masks[:-1]:
            total = total + term(m, k)
        sq[f ^ m] = total

    def square_end(m):
        sq[f ^ m] += term(m, masks[-1])

    def unit(u):
        m, q, n = u
        g = f ^ m
        i = m * subs + q
        some = pl.ds(q * height, n * height)
        for j in range(ff // tile):
            cols = pl.ds(j * tile, tile)
            active = jnp.maximum(pa_all[g, some, cols].astype(F32), 0.0)
            pre[g, some, cols] = (2.0 * active * sq[g, some, cols]).astype(BF16)
            sqr[g, some, cols] = (active * active).astype(BF16)
        total = contract_last(pre[g, some, :], up_all[...])
        for e in range(n):
            for k in range(nt):
                row, col = ((k % 2) * pr, (k // 2) * pc) if wide else (k * pr, 0)
                row += e * height
                part[k % 2, k // 2, i + e] = total[row:row + pr, col:col + pc]
        halves(u).start()

    wide = height // 2 == pr
    first_slot = lambda u: turns[u]
    slots = lambda u: pl.ds(u[0] * subs + u[1], u[2])

    def halves(u):
        i = first_slot(u)
        return remote(part.at[1 - c, :, slots(u)], from_sib.at[:, slots(u)], hs, hr.at[i], (f, t ^ 1))

    def spread(u, k):
        i = first_slot(u)
        return remote(wire.at[k, slots(u)], landed.at[k, slots(u)], ws, wr.at[i], (f, 2 * (z ^ k) + c))

    def scatter(items):
        arrived(from_sib.at[:, group_slots(items)], hr.at[turns[items[0]]])
        for u in items:
            for k in range(nz - 1, 0, -1):
                wire[k, slots(u)] = (part[c, z ^ k, slots(u)] + from_sib[z ^ k, slots(u)]).astype(BF16)
                spread(u, k).start()

    def group_slots(items):
        return pl.ds(0, sum(u[2] for u in items))

    def arrived(spot, sem):
        remote(spot, spot, hs, sem, (f, t ^ 1)).wait_recv()

    def home(u, g, k):
        return got.at[g, k, pl.ds(u[1], u[2])]

    def trade(u):
        i = first_slot(u)
        return remote(final.at[slots(u)], home(u, f, t), ts, tr.at[i], (f ^ u[0], t))

    def finish(items):
        arrived(landed.at[pl.ds(1, nz - 1), group_slots(items)], wr.at[turns[items[0]]])
        for u in items:
            value = part[c, z, slots(u)] + from_sib[z, slots(u)]
            for k in range(1, nz):
                value = value + landed[k, slots(u)].astype(F32)
            if u[0] == 0:
                got[f, t, pl.ds(u[1], u[2])] = value.astype(BF16)
            else:
                final[slots(u)] = value.astype(BF16)
                trade(u).start()

    def ring_of(u):
        i = first_slot(u)
        spot = lambda y, cls=0: home(u, f ^ u[0], 2 * y + c)
        return Gather(nz, z, lambda y: (f, 2 * y + c), lambda cls: spot(z), spot,
                      gs, lambda cls, k: gr.at[i, ahead_k.index(k) if k in ahead_k and u not in flats else len(ahead_k)],
                      ("flat",) if u in flats else ("down",))

    def over(u, k):
        spot = home(u, f ^ u[0], t ^ (2 * k))
        return remote(spot, spot, ks, kr, (f, t ^ 1))

    def announce(items):
        if items[0][0]:
            arrived(final.at[group_slots(items)], tr.at[turns[items[0]]])
        for u in items:
            outs[u] = ring_of(u)
            outs[u].push(0, 0)
            over(u, 0).start()

    def pass_on(items, steps_k, which):
        if not steps_k:
            return
        arrived(landed.at[pl.ds(0, len(steps_k)), group_slots(items)], gr.at[turns[items[0]], which])
        for k in steps_k:
            for u in items:
                outs[u].push(0, k)
                over(u, k).start()

    def down(m, first):
        g = f ^ m
        value = contract_first(sqr[g], cot_all[g, :, own_cols])
        dgrad[...] = value if first else dgrad[...] + value

    def up_part(m, first):
        g = f ^ m
        value = contract_first(inp_all[g], pre[g])
        ugrad[...] = value if first else ugrad[...] + value

    single = lambda p: p[0] in singles
    near = [p for p in inner if single(p)] + [p for p in outer if single(p)]
    far = [p for p in pairs if not single(p)]
    ahead_k = [k for k in zorder if rings[masks[0], 0].targets(0, k)]
    end_k = [k for k in zorder if k not in ahead_k]
    spots = lambda items: [p for p in items if p[1] < strips]
    near_spots, far_spots = spots(near), spots(far)

    own[0].wait()
    g_cot.push_own()
    own[1].wait()
    g_dw.push_own((0,))
    for copy in own[2:]:
        copy.start()
    take_cot(near)
    g_dw.push_own((1,))
    for m, s in near_spots[:2]:
        turn(m, s, ahead_k)
    take(g_dw, inner)
    first = (0, 0, subs)
    if subs == 1:
        steps = [[(m, 0, 1)] for m in masks]
    else:
        side = lanes // 2
        ends = lambda items, j: [(m, q, 1) for m, q in items if q in (j, lanes - 1 - j)]
        heads = [(m, q) for m in masks for q in range(lanes)]
        lead = [p for p in heads if g_pa.targets(p[1], p[0])]
        tail = [p for p in heads if p not in lead and p[0] in singles]
        deep = [p for p in heads if p not in lead and p[0] not in singles]
        steps = [ends(lead, j) for j in range(side)] + [ends(deep, j) for j in range(side)]
        steps += [[(m, q, 1) for m, q in tail if q in ((j, lanes - 1 - j) if m == singles[-1] else (lanes - 1 - j, j))]
                  for j in range(side - 1, -1, -1)]
    count = len(steps)
    turns = {u: i + 1 for i, items in enumerate(steps) for u in items}
    turns[first] = 0
    flats = [u for items in steps[-3:] for u in items]
    own[2].wait()
    g_pa.push_own((0, 1))
    take_cot(far)
    for m, s in near_spots[2:]:
        turn(m, s, ahead_k)
    for m, s in near_spots:
        turn(m, s, end_k)
    for m, s in far_spots:
        turn(m, s, ahead_k)
    take(g_dw, [p for p in outer if p[0] != masks[-1]])
    own[3].wait()
    for m in [0] + singles:
        square_start(m)
    take(g_dw, [p for p in outer if p[0] == masks[-1]])
    for copy in own[4:]:
        copy.wait()

    outs = {}

    def come(items):
        arrived(pa_all.at[0, pl.ds(0, len(items) * pah)], pa_r.at[turns[items[0]] - 1])

    def forward(items):
        for m, q, n in items:
            g_pa.push(q, m)

    def settle():
        width = cc // strips
        for m in masks:
            from_sibling(m).wait_send()
            for s in range(strips):
                rings[m, s].drain(cot_all.at[pl.ds(0, nz - 1), pl.ds(0, cr), pl.ds(0, width)])
        g_cot.drain(cot_all.at[pl.ds(0, nf - 1), pl.ds(0, cr), pl.ds(0, cc)])
        g_dw.drain(dw_all.at[:, pl.ds(0, (nf - 1) * db)])

    def swap_in(items):
        for m in items:
            exchanged(m).wait_recv()
            in_to(m).start()
            if m == deep_m:
                in_z().start()

    def fill(j):
        for job in jobs.pop(j, []):
            job()

    def refill(j):
        if subs == 1:
            if j == 0:
                for m in masks:
                    exchange(m).start()
            return
        if j < side:
            forward(steps[j])
        elif j < lanes:
            g_pa.push_own((j,))
        elif j == lanes:
            exchange(deep_m).start()
        else:
            for m in masks[:-1]:
                exchange(m, 0).start()

    groups = lambda i: [first] if i < 0 else steps[i]
    near_k = lambda items: [] if items[0] in flats else ahead_k
    rest_k = lambda items: outs[items[0]].targets(0, 0) if items[0] in flats else end_k

    def near_pass(items):
        for j, k in enumerate(near_k(items)):
            pass_on(items, [k], j)

    def rest_pass(items):
        pass_on(items, rest_k(items), len(ahead_k))

    def run(i):
        if subs > 1:
            come(steps[i])
        refill(i)
        for u in steps[i]:
            unit(u)
        if 2 <= i:
            announce(groups(i - 3))
        fill(i)
        scatter(steps[i])
        if i == 1:
            finish([first])
        if i:
            finish(steps[i - 1])
        if i >= 3 and (i < count - 1 or subs == 1):
            near_pass(groups(i - 4))

    jobs = {
        0: [lambda: square_start(masks[-1]), lambda: square_end(masks[-1])] if subs > 1 else [],
        1: [settle],
        2: [lambda: down(0, True)],
        3: [lambda: up_part(0, True)],
        4: [lambda: down(masks[-1], False)],
    }

    square_end(0)
    unit(first)
    for m in singles:
        square_end(m)
    for m, s in far_spots:
        turn(m, s, end_k)
    if subs == 1:
        for m in masks:
            if m not in singles:
                square_start(m)
                square_end(m)
        for cls in range(lanes):
            for m in masks:
                g_pa.arrive(cls, m)
                g_pa.push(cls, m)
    scatter([first])
    for i in range(count):
        run(i)
    for j in sorted(jobs):
        fill(j)
    if subs > 1:
        for m in masks[:-1]:
            exchange(m, 1).start()
    if subs > 1:
        near_pass(steps[-5])
    for m in masks if subs == 1 else singles:
        if not (subs == 1 and m == masks[-1]):
            down(m, False)
    swap_in(masks[-1:])
    announce(steps[-3])
    announce(steps[-2])
    finish(steps[-1])
    near_pass(steps[-4])
    dn_own[...] = jnp.sum(dgrad[...] * dgrad[...], axis=1).reshape(1, ff)
    downs = [remote(dn_own, dn_all.at[f], ds, dr, (f ^ m, t)) for m in range(1, nf)]
    for copy in downs:
        copy.start()
    swap_in(masks[:-1])
    announce(steps[-1])
    in_z_from().wait_recv()
    in_to_z().start()
    near_pass(steps[-3])
    for m in masks:
        in_from(m).wait_recv()
        up_part(m, False)
    un_own[...] = jnp.sum(ugrad[...] * ugrad[...], axis=1).reshape(1, db)
    ups = [remote(un_own, un_all.at[t], us, ur, (f, t ^ m)) for m in range(1, nt)]
    for copy in ups:
        copy.start()
    for items in [[first]] + steps:
        rest_pass(items)

    def up_sums():
        spot = un_all.at[pl.ds(0, nt - 1)]
        return remote(spot, spot, us, ur, (f, t ^ 1))

    def down_sums():
        spot = dn_all.at[pl.ds(0, nf - 1)]
        return remote(spot, spot, ds, dr, (f ^ 1, t))

    def norms_in():
        dn_all[f] = dn_own[...]
        un_all[t] = un_own[...]
        down_sums().wait_recv()
        up_sums().wait_recv()

    norms_in()

    def gathered():
        remote(landed, landed, ks, kr, (f, t ^ 1)).wait_recv()

    def drain():
        most = landed.at[pl.ds(1, nz - 1)]
        remote(landed, landed, ks, kr, (f, t ^ 1)).wait_send()
        remote(most, most, ws, kr, (f, t ^ 2)).wait_send()
        remote(most, most, gs, kr, (f, t ^ 2)).wait_send()
        remote(from_sib, from_sib, hs, kr, (f, t ^ 1)).wait_send()
        traded_all = final.at[pl.ds(subs, (nf - 1) * subs)]
        remote(traded_all, traded_all, ts, kr, (f ^ 1, t)).wait_send()
        for m in masks:
            exchange(m).wait_send()
            in_from(m).wait_send()
        in_z().wait_send()
        g_pa.drain(pa_all.at[pl.ds(0, nf - 1)])
        up_sums().wait_send()
        down_sums().wait_send()

    gathered()
    drain()


def fused(nf, nt, cot, dw, pa, inp, up):
    rows, d = inp.shape
    ff, db = dw.shape
    nz = nt // 2
    subs, strips = (4, 2) if nf * nz <= 64 else (1, 1)
    half = rows // subs
    pr, pc = piece_shape(nt, half, db)
    units = nf * subs
    dma = pltpu.SemaphoreType.DMA
    vmem = pl.BlockSpec(memory_space=pltpu.VMEM)
    hbm = pl.BlockSpec(memory_space=pl.ANY)
    V = pltpu.VMEM
    n = nf - 1
    cuts = share_rows(rows, nt)
    count = 7 if subs > 1 else 1 + n
    sems = [dma((3,)), dma((2, 2, n)), dma((2 * n,)), dma((n, strips)), dma((n, strips, nz - 1))]
    sems += [dma((n,)), dma((n,)), dma((nf,)), dma((nf,)), dma((n,)), dma((n,))]
    sems += [dma(()), dma((count,)), dma(()), dma((count,)), dma(()), dma((count,)), dma(()), dma((count, nz // 2))]
    sems += [dma(())] * 6 + [dma((7,))]
    return pl.pallas_call(
        functools.partial(fused_kernel, nf, nt, subs, strips),
        out_shape=[
            V((db, ff), F32), V((ff, db), F32), V((nf, nt, subs, pr, pc), BF16),
            V((nt, 1, db), F32), V((nf, 1, ff), F32),
        ],
        in_specs=[hbm] * 5,
        out_specs=[vmem] * 5,
        scratch_shapes=[
            V((rows // cuts, d * cuts // nt), BF16), V((rows, d), BF16),
            V((nf, rows, d), BF16), V((ff, d), BF16), V((nf, rows, ff), BF16), V((nf, rows, db), BF16),
            V((db, ff), BF16), V((nf, rows, ff), BF16), V((nf, rows, ff), BF16), V((nf, rows, ff), F32),
            V((2, nz, units, pr, pc), F32), V((nz, units, pr, pc), F32),
            V((nz, units, pr, pc), BF16), V((nz, units, pr, pc), BF16), V((units, pr, pc), BF16),
            V((1, db), F32), V((1, ff), F32),
        ] + sems,
        compiler_params=pltpu.CompilerParams(has_side_effects=True, collective_id=0, vmem_limit_bytes=54 * 2 ** 20),
    )(cot, dw, pa, inp, up)


def deliver_kernel(ugrad, dgrad, got, un_all, dn_all, ug_out, dg_out, out, un_out, dn_out, whole, un_sum, dn_sum, sem):
    nf, nt, subs, pr, pc = got.shape
    rows, d = whole.shape
    half, db = rows // subs, d // nf
    copies = [pltpu.make_async_copy(ugrad, ug_out, sem.at[3]), pltpu.make_async_copy(dgrad, dg_out, sem.at[4])]
    for copy in copies:
        copy.start()
    wide = half // 2 == pr
    for h in range(subs):
        for k in range(nt):
            for g in range(nf):
                row, col = ((k % 2) * pr, (k // 2) * pc) if wide else (k * pr, 0)
                whole[h * half + row:h * half + row + pr, g * db + col:g * db + col + pc] = got[g, k, h]
    un, dn = un_all[0], dn_all[0]
    for k in range(1, nt):
        un = un + un_all[k]
    for k in range(1, nf):
        dn = dn + dn_all[k]
    un_sum[...] = un
    dn_sum[...] = dn
    last = [pltpu.make_async_copy(whole, out, sem.at[0]), pltpu.make_async_copy(un_sum, un_out, sem.at[1]),
            pltpu.make_async_copy(dn_sum, dn_out, sem.at[2])]
    for copy in last:
        copy.start()
    for copy in copies + last:
        copy.wait()


def deliver(rows, d, ugrad, dgrad, got, un_all, dn_all):
    hbm, vmem = pl.BlockSpec(memory_space=pl.ANY), pl.BlockSpec(memory_space=pltpu.VMEM)
    V = pltpu.VMEM
    un, dn = un_all.shape[1:], dn_all.shape[1:]
    H = jax.ShapeDtypeStruct
    return pl.pallas_call(
        deliver_kernel,
        out_shape=[H(ugrad.shape, F32), H(dgrad.shape, F32), H((rows, d), BF16), H(un, F32), H(dn, F32)],
        in_specs=[vmem] * 5,
        out_specs=[hbm] * 5,
        scratch_shapes=[V((rows, d), BF16), V(un, F32), V(dn, F32), pltpu.SemaphoreType.DMA((5,))],
        compiler_params=pltpu.CompilerParams(vmem_limit_bytes=16 * 2 ** 20),
    )(ugrad, dgrad, got, un_all, dn_all)


def local(nf, nt, inputs, pre_act, cotangent, up_weight, down_weight):
    db, ff = up_weight.shape
    parts = fused(nf, nt, cotangent, down_weight, pre_act, inputs, up_weight)
    up_grad, down_grad, out, un, dn = deliver(*inputs.shape, *parts)
    return out, up_grad, down_grad, un.reshape(db), dn.reshape(ff)


def solution(mesh):
    in_specs = (P("fs", None), P("fs", "tp"), P("fs", None), P("fs", "tp"), P("tp", "fs"))
    out_specs = (P("fs", None), P("fs", "tp"), P("tp", "fs"), P("fs"), P("tp"))
    body = functools.partial(local, mesh.shape["fs"], mesh.shape["tp"])
    return jax.shard_map(body, mesh=mesh, in_specs=in_specs, out_specs=out_specs, check_vma=False)
```

```python
import functools

import jax
import jax.numpy as jnp
from jax import lax
from jax.experimental import pallas as pl
from jax.experimental.pallas import tpu as pltpu
from jax.sharding import PartitionSpec as P

MESH = pl.DeviceIdType.MESH
F32, BF16 = jnp.float32, jnp.bfloat16


def contract_last(left, right):
    return lax.dot_general(left, right, (((1,), (1,)), ((), ())), preferred_element_type=F32)


def contract_first(left, right):
    return lax.dot_general(left, right, (((0,), (0,)), ((), ())), preferred_element_type=F32)


def bits_of(n):
    return [1 << i for i in range(n.bit_length() - 1)]


def by_weight(n, down=False):
    return sorted(range(1, n), key=lambda m: (bin(m).count("1"), -m if down else m))


class Gather:
    def __init__(self, n, me, device, source, place, send, recv, orders):
        self.n, self.me, self.device = n, me, device
        self.source, self.place = source, place
        self.send, self.recv, self.orders = send, recv, orders

    def targets(self, cls, m):
        bits = bits_of(self.n)
        if self.orders[cls] == "flat":
            return list(range(self.n - 1, 0, -1)) if m == 0 else []
        if m == 0:
            return bits
        if self.orders[cls] == "up":
            return [b for b in bits if b > m]
        return [b for b in bits if b < (m & -m)]

    def copy(self, cls, m, b):
        there = self.place(self.me ^ m, cls)
        return pltpu.make_async_remote_copy(
            src_ref=self.source(cls) if m == 0 else there,
            dst_ref=there,
            send_sem=self.send,
            recv_sem=self.recv(cls, m ^ b),
            device_id=self.device(self.me ^ b),
            device_id_type=MESH,
        )

    def push(self, cls, m, only=None):
        for b in self.targets(cls, m):
            if only is None or b == only:
                self.copy(cls, m, b).start()

    def push_own(self, turns=None):
        classes = list(range(len(self.orders)))
        for i, b in enumerate(bits_of(self.n)):
            for j, cls in enumerate(classes if i % 2 == 0 else classes[::-1]):
                if turns is None or j in turns:
                    self.push(cls, 0, b)

    def arrive(self, cls, m):
        here = self.place(self.me ^ m, cls)
        pltpu.make_async_remote_copy(
            src_ref=here,
            dst_ref=here,
            send_sem=self.send,
            recv_sem=self.recv(cls, m),
            device_id=self.device(self.me ^ (m & -m)),
            device_id_type=MESH,
        ).wait_recv()

    def drain(self, sent):
        pltpu.make_async_remote_copy(src_ref=sent, dst_ref=sent, send_sem=self.send, recv_sem=self.send,
                                     device_id=self.device(self.me ^ 1), device_id_type=MESH).wait_send()


def share_rows(rows, parts):
    cuts = 1
    while cuts < parts and rows % (2 * cuts * 16) == 0:
        cuts *= 2
    return cuts


def piece_shape(nt, rows, db):
    nz = nt // 2
    if db % (128 * nz) == 0:
        return rows // 2, db // nz
    return rows // nt, db


def fused_kernel(nf, nt, subs, strips, cot, dw, pa, inp, up, ugrad, dgrad, got, un_all, dn_all,
                 cot_own, inp_own, cot_all, dw_all, pa_all, inp_all, up_all, pre, sqr, sq,
                 part, from_sib, wire, landed, final, un_own, dn_own,
                 xs, xr, pa_r, zs, zr, ss, sr, a_s, a_r, bs, br, hs, hr, ws, wr, ts, tr, gs, gr, ks, kr,
                 us, ur, ds, dr, local_sem):
    f, t = lax.axis_index("fs"), lax.axis_index("tp")
    z, c = t // 2, t % 2
    nz = nt // 2
    rows, d = cot.shape
    ff, db = dw.shape
    height = rows // subs
    pr, pc = part.shape[3:]
    own_cols = pl.ds(pl.multiple_of(f * db, db), db)

    def remote(src, dst, send, recv, device):
        return pltpu.make_async_remote_copy(src_ref=src, dst_ref=dst, send_sem=send, recv_sem=recv,
                                            device_id=device, device_id_type=MESH)

    ih = rows // 2

    def columns(g, side):
        return inp.at[pl.ds(pl.multiple_of(side * ih, ih), ih), pl.ds(pl.multiple_of(g * db, db), db)]

    def in_half(g, side):
        return inp_all.at[g, pl.ds(pl.multiple_of(side * ih, ih), ih), :]

    row_cuts = share_rows(rows, nt)
    col_cuts = nt // row_cuts
    cr, cc = rows // row_cuts, d // col_cuts
    first_piece = cot.at[pl.ds(pl.multiple_of((t // col_cuts) * cr, cr), cr),
                         pl.ds(pl.multiple_of((t % col_cuts) * cc, cc), cc)]
    own = [
        pltpu.make_async_copy(first_piece, cot_own, local_sem.at[0]),
        pltpu.make_async_copy(dw, dw_all.at[:, own_cols], local_sem.at[1]),
        pltpu.make_async_copy(pa, pa_all.at[f], local_sem.at[2]),
        pltpu.make_async_copy(cot, cot_all.at[f], local_sem.at[3]),
        pltpu.make_async_copy(up, up_all, local_sem.at[4]),
        pltpu.make_async_copy(inp.at[:, own_cols], inp_all.at[f], local_sem.at[5]),
        pltpu.make_async_copy(inp, inp_own, local_sem.at[6]),
    ]
    for copy in own[:2]:
        copy.start()

    barrier = pltpu.get_barrier_semaphore()
    peers = [(f ^ m, t) for m in range(1, nf)] + [(f, t ^ m) for m in range(1, nt)]
    for peer in peers:
        pl.semaphore_signal(barrier, inc=1, device_id=peer, device_id_type=MESH)
    pl.semaphore_wait(barrier, len(peers))

    def piece(ref, y, h=None):
        row = pl.multiple_of((y // col_cuts) * cr, cr)
        width = cc if h is None else cc // 2
        col = (y % col_cuts) * cc + (0 if h is None else h * width)
        return ref.at[pl.ds(row, cr), pl.ds(pl.multiple_of(col, width), width)]

    dwh = ff // 2
    lanes = max(subs, 2)
    pah = rows // lanes

    def pa_turn(cls, m):
        return cls * (nf - 1) + m - 1 if subs == 1 else turns[m, cls, 1] - 1

    def over_fs(k, source, place, n=2):
        return Gather(nf, f, lambda g: (g, t), source, place, xs.at[k],
                      lambda cls, m: pa_r.at[pa_turn(cls, m)] if k == 2 else xr.at[k, cls, m - 1],
                      ("up",) * (n // 2) + ("down",) * (n // 2))

    g_cot = over_fs(0, lambda h: cot_own.at[:, pl.ds(h * (cc // 2), cc // 2)], lambda g, h: piece(cot_all.at[g], t, h))
    g_dw = over_fs(1, lambda h: dw_all.at[pl.ds(h * dwh, dwh), own_cols],
                   lambda g, h: dw_all.at[pl.ds(h * dwh, dwh), pl.ds(pl.multiple_of(g * db, db), db)])
    g_pa = over_fs(2, lambda h: pa_all.at[f, pl.ds(h * pah, pah), :],
                   lambda g, h: pa_all.at[g, pl.ds(h * pah, pah), :], lanes)

    def strip(m, s, y):
        return piece(cot_all.at[f ^ m], y, s if strips == 2 else None)

    def over_z(m, s):
        spot = lambda y, cls=0: strip(m, s, 2 * y + c)
        return Gather(nz, z, lambda y: (f, 2 * y + c), lambda cls: spot(z), spot,
                      zs.at[m - 1, s], lambda cls, k: zr.at[m - 1, s, k - 1], ("down",))

    def to_sibling(m, s, k):
        spot = strip(m, s, 2 * (z ^ k) + c)
        return remote(spot, spot, ss.at[m - 1], sr.at[m - 1], (f, t ^ 1))

    def from_sibling(m):
        spot = cot_all.at[pl.ds(0, nz), pl.ds(0, cr), pl.ds(0, cc)]
        return remote(spot, spot, ss.at[m - 1], sr.at[m - 1], (f, t ^ 1))

    iq = rows // 4
    seat = lambda y: (2 * y + c)

    def quarter(g, q):
        return inp_all.at[g, pl.ds(pl.multiple_of(q * iq, iq), iq), :]

    def source(m):
        height, q = (iq, seat(z % 2)) if m == deep_m else (ih, c)
        return inp_own.at[pl.ds(pl.multiple_of(q * height, height), height), pl.ds(pl.multiple_of((f ^ m) * db, db), db)]

    def place(m, g):
        return quarter(g, seat(z % 2)) if m == deep_m else in_half(g, c)

    def exchange(m, part=None):
        src, dst = source(m), place(m, f)
        if part is not None:
            src, dst = src.at[pl.ds(part * iq, iq)], dst.at[pl.ds(part * iq, iq)]
        return remote(src, dst, a_s.at[m - 1], a_r.at[m - 1], (f ^ m, t))

    exchanged = lambda m: remote(place(m, f ^ m), place(m, f ^ m), a_s.at[m - 1], a_r.at[m - 1], (f ^ m, t))
    in_to = lambda m: remote(place(m, f ^ m), place(m, f ^ m), bs.at[m - 1], br.at[m - 1], (f, t ^ 1))

    def in_from(m):
        return remote(in_half(f ^ m, 1 - c), in_half(f ^ m, 1 - c), bs.at[m - 1], br.at[m - 1], (f, t ^ 1))

    def in_z():
        spot = quarter(f ^ deep_m, seat(z % 2))
        return remote(spot, spot, a_s.at[nf - 1], a_r.at[nf - 1], (f, t ^ 2))

    def in_z_from():
        spot = quarter(f ^ deep_m, seat(1 - z % 2))
        return remote(spot, spot, a_s.at[nf - 1], a_r.at[nf - 1], (f, t ^ 2))

    def in_to_z():
        spot = quarter(f ^ deep_m, seat(1 - z % 2))
        return remote(spot, spot, bs.at[deep_m - 1], br.at[deep_m - 1], (f, t ^ 1))

    masks = by_weight(nf)
    deep_m = masks[-1]
    zorder = by_weight(nz, True)
    left = {m: 2 for m in masks}
    rings = {(m, s): over_z(m, s) for m in masks for s in range(strips)}
    singles = [m for m in masks if m & (m - 1) == 0]
    pairs = [(m, cls) for m in masks for cls in (0, 1)]
    inner = [p for p in pairs if g_dw.targets(p[1], p[0])]
    outer = [p for p in pairs if p not in inner]

    def take_cot(items):
        for m, cls in items:
            g_cot.arrive(cls, m)
            g_cot.push(cls, m)
            left[m] -= 1
            if strips == 2:
                rings[m, cls].push(0, 0)
                to_sibling(m, cls, 0).start()
            elif left[m] == 0:
                rings[m, 0].push(0, 0)
                to_sibling(m, 0, 0).start()

    def turn(m, s, steps):
        for k in steps:
            rings[m, s].arrive(0, k)
            rings[m, s].push(0, k)
            to_sibling(m, s, k).start()

    def take(g, items):
        for m, cls in items:
            g.arrive(cls, m)
            g.push(cls, m)

    tile = min(ff, 256)

    def term(m, k):
        cols = pl.ds(pl.multiple_of((f ^ k) * db, db), db)
        return contract_last(cot_all[f ^ m, :, cols], dw_all[:, cols])

    def square_start(m):
        if m:
            from_sibling(m).wait_recv()
        total = term(m, 0)
        for k in masks[:-1]:
            total = total + term(m, k)
        sq[f ^ m] = total

    def square_end(m):
        sq[f ^ m] += term(m, masks[-1])

    def unit(u):
        m, q, n = u
        g = f ^ m
        i = m * subs + q
        some = pl.ds(q * height, n * height)
        for j in range(ff // tile):
            cols = pl.ds(j * tile, tile)
            active = jnp.maximum(pa_all[g, some, cols].astype(F32), 0.0)
            pre[g, some, cols] = (2.0 * active * sq[g, some, cols]).astype(BF16)
            sqr[g, some, cols] = (active * active).astype(BF16)
        total = contract_last(pre[g, some, :], up_all[...])
        for e in range(n):
            for k in range(nt):
                row, col = ((k % 2) * pr, (k // 2) * pc) if wide else (k * pr, 0)
                row += e * height
                part[k % 2, k // 2, i + e] = total[row:row + pr, col:col + pc]
        halves(u).start()

    wide = height // 2 == pr
    first_slot = lambda u: turns[u]
    slots = lambda u: pl.ds(u[0] * subs + u[1], u[2])

    def halves(u):
        i = first_slot(u)
        return remote(part.at[1 - c, :, slots(u)], from_sib.at[:, slots(u)], hs, hr.at[i], (f, t ^ 1))

    def spread(u, k):
        i = first_slot(u)
        return remote(wire.at[k, slots(u)], landed.at[k, slots(u)], ws, wr.at[i], (f, 2 * (z ^ k) + c))

    def scatter(items):
        arrived(from_sib.at[:, group_slots(items)], hr.at[turns[items[0]]])
        for u in items:
            for k in range(nz - 1, 0, -1):
                wire[k, slots(u)] = (part[c, z ^ k, slots(u)] + from_sib[z ^ k, slots(u)]).astype(BF16)
                spread(u, k).start()

    def group_slots(items):
        return pl.ds(0, sum(u[2] for u in items))

    def arrived(spot, sem):
        remote(spot, spot, hs, sem, (f, t ^ 1)).wait_recv()

    def home(u, g, k):
        return got.at[g, k, pl.ds(u[1], u[2])]

    def trade(u):
        i = first_slot(u)
        return remote(final.at[slots(u)], home(u, f, t), ts, tr.at[i], (f ^ u[0], t))

    def finish(items):
        arrived(landed.at[pl.ds(1, nz - 1), group_slots(items)], wr.at[turns[items[0]]])
        for u in items:
            value = part[c, z, slots(u)] + from_sib[z, slots(u)]
            for k in range(1, nz):
                value = value + landed[k, slots(u)].astype(F32)
            if u[0] == 0:
                got[f, t, pl.ds(u[1], u[2])] = value.astype(BF16)
            else:
                final[slots(u)] = value.astype(BF16)
                trade(u).start()

    def ring_of(u):
        i = first_slot(u)
        spot = lambda y, cls=0: home(u, f ^ u[0], 2 * y + c)
        return Gather(nz, z, lambda y: (f, 2 * y + c), lambda cls: spot(z), spot,
                      gs, lambda cls, k: gr.at[i, ahead_k.index(k) if k in ahead_k and u not in flats else len(ahead_k)],
                      ("flat",) if u in flats else ("down",))

    def over(u, k):
        spot = home(u, f ^ u[0], t ^ (2 * k))
        return remote(spot, spot, ks, kr, (f, t ^ 1))

    def announce(items):
        if items[0][0]:
            arrived(final.at[group_slots(items)], tr.at[turns[items[0]]])
        for u in items:
            outs[u] = ring_of(u)
            outs[u].push(0, 0)
            over(u, 0).start()

    def pass_on(items, steps_k, which):
        if not steps_k:
            return
        arrived(landed.at[pl.ds(0, len(steps_k)), group_slots(items)], gr.at[turns[items[0]], which])
        for k in steps_k:
            for u in items:
                outs[u].push(0, k)
                over(u, k).start()

    def stacked(items, read):
        values = [read(f ^ m) for m in items]
        return values[0] if len(values) == 1 else jnp.concatenate(values, axis=0)

    def down(items, first=False):
        value = contract_first(stacked(items, lambda g: sqr[g]), stacked(items, lambda g: cot_all[g, :, own_cols]))
        dgrad[...] = value if first else dgrad[...] + value

    def up_part(items, first=False):
        value = contract_first(stacked(items, lambda g: inp_all[g]), stacked(items, lambda g: pre[g]))
        ugrad[...] = value if first else ugrad[...] + value

    single = lambda p: p[0] in singles
    near = [p for p in inner if single(p)] + [p for p in outer if single(p)]
    far = [p for p in pairs if not single(p)]
    ahead_k = [k for k in zorder if rings[masks[0], 0].targets(0, k)]
    end_k = [k for k in zorder if k not in ahead_k]
    spots = lambda items: [p for p in items if p[1] < strips]
    near_spots, far_spots = spots(near), spots(far)

    own[0].wait()
    g_cot.push_own()
    own[1].wait()
    g_dw.push_own((0,))
    for copy in own[2:]:
        copy.start()
    take_cot(near)
    g_dw.push_own((1,))
    for m, s in near_spots[:2]:
        turn(m, s, ahead_k)
    take(g_dw, inner)
    first = (0, 0, subs)
    if subs == 1:
        steps = [[(m, 0, 1)] for m in masks]
    else:
        side = lanes // 2
        ends = lambda items, j: [(m, q, 1) for m, q in items if q in (j, lanes - 1 - j)]
        heads = [(m, q) for m in masks for q in range(lanes)]
        lead = [p for p in heads if g_pa.targets(p[1], p[0])]
        tail = [p for p in heads if p not in lead and p[0] in singles]
        deep = [p for p in heads if p not in lead and p[0] not in singles]
        steps = [ends(lead, j) for j in range(side)] + [ends(deep, j) for j in range(side)]
        steps += [[(m, q, 1) for m, q in tail if q in ((j, lanes - 1 - j) if m == singles[-1] else (lanes - 1 - j, j))]
                  for j in range(side - 1, -1, -1)]
    count = len(steps)
    turns = {u: i + 1 for i, items in enumerate(steps) for u in items}
    turns[first] = 0
    flats = [u for items in steps[-3:] for u in items]
    own[2].wait()
    g_pa.push_own((0, 1))
    take_cot(far)
    for m, s in near_spots[2:]:
        turn(m, s, ahead_k)
    for m, s in near_spots:
        turn(m, s, end_k)
    for m, s in far_spots:
        turn(m, s, ahead_k)
    take(g_dw, [p for p in outer if p[0] != masks[-1]])
    own[3].wait()
    for m in [0] + singles:
        square_start(m)
    take(g_dw, [p for p in outer if p[0] == masks[-1]])
    for copy in own[4:]:
        copy.wait()

    outs = {}

    def come(items):
        arrived(pa_all.at[0, pl.ds(0, len(items) * pah)], pa_r.at[turns[items[0]] - 1])

    def forward(items):
        for m, q, n in items:
            g_pa.push(q, m)

    def settle():
        width = cc // strips
        for m in masks:
            from_sibling(m).wait_send()
            for s in range(strips):
                rings[m, s].drain(cot_all.at[pl.ds(0, nz - 1), pl.ds(0, cr), pl.ds(0, width)])
        g_cot.drain(cot_all.at[pl.ds(0, nf - 1), pl.ds(0, cr), pl.ds(0, cc)])
        g_dw.drain(dw_all.at[:, pl.ds(0, (nf - 1) * db)])

    def swap_in(items):
        for m in items:
            exchanged(m).wait_recv()
            in_to(m).start()
            if m == deep_m:
                in_z().start()

    def fill(j):
        for job in jobs.pop(j, []):
            job()

    def refill(j):
        if subs == 1:
            if j == 0:
                for m in masks:
                    exchange(m).start()
            return
        if j < side:
            forward(steps[j])
        elif j < lanes:
            g_pa.push_own((j,))
        elif j == lanes:
            exchange(deep_m).start()
        else:
            for m in masks[:-1]:
                exchange(m, 0).start()

    groups = lambda i: [first] if i < 0 else steps[i]
    near_k = lambda items: [] if items[0] in flats else ahead_k
    rest_k = lambda items: outs[items[0]].targets(0, 0) if items[0] in flats else end_k

    def near_pass(items):
        for j, k in enumerate(near_k(items)):
            pass_on(items, [k], j)

    def rest_pass(items):
        pass_on(items, rest_k(items), len(ahead_k))

    def run(i):
        if subs > 1:
            come(steps[i])
        refill(i)
        for u in steps[i]:
            unit(u)
        if 2 <= i:
            announce(groups(i - 3))
        fill(i)
        scatter(steps[i])
        if i == 1:
            finish([first])
        if i:
            finish(steps[i - 1])
        if i >= 3 and (i < count - 1 or subs == 1):
            near_pass(groups(i - 4))

    jobs = {
        0: [lambda: square_start(masks[-1]), lambda: square_end(masks[-1])] if subs > 1 else [],
        1: [settle],
        2: [lambda: down([0], True)],
        3: [lambda: up_part([0], True)],
        4: [lambda: down([masks[-1]])],
    }

    square_end(0)
    unit(first)
    for m in singles:
        square_end(m)
    for m, s in far_spots:
        turn(m, s, end_k)
    if subs == 1:
        for m in masks:
            if m not in singles:
                square_start(m)
                square_end(m)
        for cls in range(lanes):
            for m in masks:
                g_pa.arrive(cls, m)
                g_pa.push(cls, m)
    scatter([first])
    for i in range(count):
        run(i)
    for j in sorted(jobs):
        fill(j)
    if subs > 1:
        for m in masks[:-1]:
            exchange(m, 1).start()
    if subs > 1:
        near_pass(steps[-5])
    swap_in(masks[-1:])
    announce(steps[-3])
    announce(steps[-2])
    rest = masks[:-1] if subs == 1 else singles
    for j in range(0, len(rest), 2):
        down(rest[j:j + 2])
    finish(steps[-1])
    near_pass(steps[-4])
    dn_own[...] = jnp.sum(dgrad[...] * dgrad[...], axis=1).reshape(1, ff)
    downs = [remote(dn_own, dn_all.at[f], ds, dr, (f ^ m, t)) for m in range(1, nf)]
    for copy in downs:
        copy.start()
    swap_in(masks[:-1])
    announce(steps[-1])
    in_z_from().wait_recv()
    in_to_z().start()
    near_pass(steps[-3])
    for j in range(0, len(masks), 2):
        for m in masks[j:j + 2]:
            in_from(m).wait_recv()
        up_part(masks[j:j + 2])
    un_own[...] = jnp.sum(ugrad[...] * ugrad[...], axis=1).reshape(1, db)
    ups = [remote(un_own, un_all.at[t], us, ur, (f, t ^ m)) for m in range(1, nt)]
    for copy in ups:
        copy.start()
    for items in [[first]] + steps:
        rest_pass(items)

    def up_sums():
        spot = un_all.at[pl.ds(0, nt - 1)]
        return remote(spot, spot, us, ur, (f, t ^ 1))

    def down_sums():
        spot = dn_all.at[pl.ds(0, nf - 1)]
        return remote(spot, spot, ds, dr, (f ^ 1, t))

    def norms_in():
        dn_all[f] = dn_own[...]
        un_all[t] = un_own[...]
        down_sums().wait_recv()
        up_sums().wait_recv()

    norms_in()

    def gathered():
        remote(landed, landed, ks, kr, (f, t ^ 1)).wait_recv()

    def drain():
        most = landed.at[pl.ds(1, nz - 1)]
        remote(landed, landed, ks, kr, (f, t ^ 1)).wait_send()
        remote(most, most, ws, kr, (f, t ^ 2)).wait_send()
        remote(most, most, gs, kr, (f, t ^ 2)).wait_send()
        remote(from_sib, from_sib, hs, kr, (f, t ^ 1)).wait_send()
        traded_all = final.at[pl.ds(subs, (nf - 1) * subs)]
        remote(traded_all, traded_all, ts, kr, (f ^ 1, t)).wait_send()
        for m in masks:
            exchange(m).wait_send()
            in_from(m).wait_send()
        in_z().wait_send()
        g_pa.drain(pa_all.at[pl.ds(0, nf - 1)])
        up_sums().wait_send()
        down_sums().wait_send()

    gathered()
    drain()


def fused(nf, nt, cot, dw, pa, inp, up):
    rows, d = inp.shape
    ff, db = dw.shape
    nz = nt // 2
    subs, strips = (4, 2) if nf * nz <= 64 else (1, 1)
    half = rows // subs
    pr, pc = piece_shape(nt, half, db)
    units = nf * subs
    dma = pltpu.SemaphoreType.DMA
    vmem = pl.BlockSpec(memory_space=pltpu.VMEM)
    hbm = pl.BlockSpec(memory_space=pl.ANY)
    V = pltpu.VMEM
    n = nf - 1
    cuts = share_rows(rows, nt)
    count = 7 if subs > 1 else 1 + n
    sems = [dma((3,)), dma((2, 2, n)), dma((2 * n,)), dma((n, strips)), dma((n, strips, nz - 1))]
    sems += [dma((n,)), dma((n,)), dma((nf,)), dma((nf,)), dma((n,)), dma((n,))]
    sems += [dma(()), dma((count,)), dma(()), dma((count,)), dma(()), dma((count,)), dma(()), dma((count, nz // 2))]
    sems += [dma(())] * 6 + [dma((7,))]
    return pl.pallas_call(
        functools.partial(fused_kernel, nf, nt, subs, strips),
        out_shape=[
            V((db, ff), F32), V((ff, db), F32), V((nf, nt, subs, pr, pc), BF16),
            V((nt, 1, db), F32), V((nf, 1, ff), F32),
        ],
        in_specs=[hbm] * 5,
        out_specs=[vmem] * 5,
        scratch_shapes=[
            V((rows // cuts, d * cuts // nt), BF16), V((rows, d), BF16),
            V((nf, rows, d), BF16), V((ff, d), BF16), V((nf, rows, ff), BF16), V((nf, rows, db), BF16),
            V((db, ff), BF16), V((nf, rows, ff), BF16), V((nf, rows, ff), BF16), V((nf, rows, ff), F32),
            V((2, nz, units, pr, pc), F32), V((nz, units, pr, pc), F32),
            V((nz, units, pr, pc), BF16), V((nz, units, pr, pc), BF16), V((units, pr, pc), BF16),
            V((1, db), F32), V((1, ff), F32),
        ] + sems,
        compiler_params=pltpu.CompilerParams(has_side_effects=True, collective_id=0, vmem_limit_bytes=54 * 2 ** 20),
    )(cot, dw, pa, inp, up)


def deliver_kernel(ugrad, dgrad, got, un_all, dn_all, ug_out, dg_out, out, un_out, dn_out, whole, un_sum, dn_sum, sem):
    nf, nt, subs, pr, pc = got.shape
    rows, d = whole.shape
    half, db = rows // subs, d // nf
    copies = [pltpu.make_async_copy(ugrad, ug_out, sem.at[3]), pltpu.make_async_copy(dgrad, dg_out, sem.at[4])]
    for copy in copies:
        copy.start()
    wide = half // 2 == pr
    for h in range(subs):
        for k in range(nt):
            for g in range(nf):
                row, col = ((k % 2) * pr, (k // 2) * pc) if wide else (k * pr, 0)
                whole[h * half + row:h * half + row + pr, g * db + col:g * db + col + pc] = got[g, k, h]
    un, dn = un_all[0], dn_all[0]
    for k in range(1, nt):
        un = un + un_all[k]
    for k in range(1, nf):
        dn = dn + dn_all[k]
    un_sum[...] = un
    dn_sum[...] = dn
    last = [pltpu.make_async_copy(whole, out, sem.at[0]), pltpu.make_async_copy(un_sum, un_out, sem.at[1]),
            pltpu.make_async_copy(dn_sum, dn_out, sem.at[2])]
    for copy in last:
        copy.start()
    for copy in copies + last:
        copy.wait()


def deliver(rows, d, ugrad, dgrad, got, un_all, dn_all):
    hbm, vmem = pl.BlockSpec(memory_space=pl.ANY), pl.BlockSpec(memory_space=pltpu.VMEM)
    V = pltpu.VMEM
    un, dn = un_all.shape[1:], dn_all.shape[1:]
    H = jax.ShapeDtypeStruct
    return pl.pallas_call(
        deliver_kernel,
        out_shape=[H(ugrad.shape, F32), H(dgrad.shape, F32), H((rows, d), BF16), H(un, F32), H(dn, F32)],
        in_specs=[vmem] * 5,
        out_specs=[hbm] * 5,
        scratch_shapes=[V((rows, d), BF16), V(un, F32), V(dn, F32), pltpu.SemaphoreType.DMA((5,))],
        compiler_params=pltpu.CompilerParams(vmem_limit_bytes=16 * 2 ** 20),
    )(ugrad, dgrad, got, un_all, dn_all)


def local(nf, nt, inputs, pre_act, cotangent, up_weight, down_weight):
    db, ff = up_weight.shape
    parts = fused(nf, nt, cotangent, down_weight, pre_act, inputs, up_weight)
    up_grad, down_grad, out, un, dn = deliver(*inputs.shape, *parts)
    return out, up_grad, down_grad, un.reshape(db), dn.reshape(ff)


def solution(mesh):
    in_specs = (P("fs", None), P("fs", "tp"), P("fs", None), P("fs", "tp"), P("tp", "fs"))
    out_specs = (P("fs", None), P("fs", "tp"), P("tp", "fs"), P("fs"), P("tp"))
    body = functools.partial(local, mesh.shape["fs"], mesh.shape["tp"])
    return jax.shard_map(body, mesh=mesh, in_specs=in_specs, out_specs=out_specs, check_vma=False)
```
